32 devices in a mesh: ra: 8 (over z, y), cb: 4 (over x, core).
Axes of the slice: x: 2, y: 2, z: 4, core: 2. Of those that a mesh axis runs over, the one named last changes fastest.
Arguments:
- tokens: bfloat16 [4, 128, 4096], P(None, None, 'ra'), may hold values from -64 to 64
- norm_gain: float32 [2, 4096], P(None, 'ra'), may hold values from 0.1 to 1.9
- gate_weight: bfloat16 [2, 4096, 11264], P(None, 'ra', 'cb'), may hold values from -0.09375 to 0.09375
- up_weight: bfloat16 [2, 4096, 11264], P(None, 'ra', 'cb'), may hold values from -0.09375 to 0.09375
- gate_taps: float32 [2, 3, 11264], P(None, None, 'cb'), may hold values from -3 to 3
- up_taps: float32 [2, 3, 11264], P(None, None, 'cb'), may hold values from -3 to 3
- gate_bias: float32 [2, 11264], P(None, 'cb'), may hold values from -3 to 3
- up_bias: float32 [2, 11264], P(None, 'cb'), may hold values from -3 to 3
- down_weight: bfloat16 [2, 11264, 4096], P(None, 'cb', 'ra'), may hold values from -0.0546875 to 0.0546875
Outputs:
- mixed: bfloat16 [4, 128, 4096], P(None, None, 'ra')
The draws below stay inside these ranges and needn't reach their ends.
All inputs are finite; a program needn't handle non-finite values.
Results may differ from the reference program's by a relative error of at most 0.03.
Values may be sent and summed in bfloat16 or wider, within the bound.
A program may use at most 64 MiB of HBM per device.

```python
import jax
import jax.numpy as jnp
from jax import lax

D = 4096
FF = 11264
KERNEL = 3
LAYERS = 2
SEQS = 4
LEN = 128


def draw_tokens(key, part):
    key_base, key_scale, key_rows, key_common = jax.random.split(key, 4)
    width = D // 32
    noise = jnp.clip(jax.random.normal(key_base, (SEQS, LEN, D), jnp.float32), -6.0, 6.0)
    row_scale = jnp.exp(jax.random.uniform(key_rows, (SEQS, LEN, 1), jnp.float32, -0.5, 0.5))
    scales = jnp.exp(jax.random.uniform(key_scale, (32,), jnp.float32, -1.4, 1.4))
    columns = jnp.repeat(scales, width)
    return jnp.clip(noise * columns * row_scale, -64.0, 64.0).astype(jnp.bfloat16)


def block_scale(rng, shape, cuts, least, largest):
    loudness = 1.0
    for position, parts in cuts:
        heights = jax.random.uniform(jax.random.fold_in(jax.random.fold_in(rng, 6), position), (parts,), jnp.float32, least / len(cuts), largest / len(cuts))
        loudness = loudness * jnp.repeat(jnp.exp(heights), shape[position] // parts).reshape((-1,) + (1,) * (len(shape) - 1 - position))
    return loudness


def centred(stream_key, shape, deviation, most, shards=(), dtype=jnp.bfloat16):
    gain = block_scale(stream_key, shape, shards, -0.22, 0.18) if shards else 1.0
    values = jax.random.normal(stream_key, shape, jnp.float32) * deviation * gain
    return jnp.minimum(jnp.maximum(values, -most), most).astype(dtype)


def setup_inputs(seed: int = 0) -> dict:
    arg_keys = jax.random.split(jax.random.key(seed), 10)
    tokens = draw_tokens(jax.random.fold_in(arg_keys[9], 71), 0)
    norm_gain = jnp.clip(1.0 + 0.18 * jax.random.normal(arg_keys[1], (LAYERS, D), jnp.float32), 0.1, 1.9)
    gate_weight = centred(arg_keys[2], (LAYERS, D, FF), D ** -0.5, 0.09375, ((1, 8), (2, 4)))
    up_weight = centred(arg_keys[3], (LAYERS, D, FF), D ** -0.5, 0.09375, ((1, 8), (2, 4)))
    gate_taps = centred(arg_keys[4], (LAYERS, KERNEL, FF), 0.6, 3.0, ((2, 4),), jnp.float32)
    up_taps = centred(arg_keys[5], (LAYERS, KERNEL, FF), 0.6, 3.0, ((2, 4),), jnp.float32)
    gate_bias = centred(arg_keys[6], (LAYERS, FF), 0.5, 3.0, ((1, 4),), jnp.float32)
    up_bias = centred(arg_keys[7], (LAYERS, FF), 0.5, 3.0, ((1, 4),), jnp.float32)
    down_weight = centred(arg_keys[8], (LAYERS, FF, D), FF ** -0.5, 0.0546875, ((1, 4), (2, 8)))
    return {"tokens": tokens, "norm_gain": norm_gain, "gate_weight": gate_weight, "up_weight": up_weight, "gate_taps": gate_taps, "up_taps": up_taps, "gate_bias": gate_bias, "up_bias": up_bias, "down_weight": down_weight}


eps = 1e-06
resid_scale = 0.5

def causal_conv(projected, kernel, offsets):
    values = projected.astype(jnp.float32).reshape(SEQS, LEN, FF)
    padded = jnp.pad(values, ((0, 0), (KERNEL - 1, 0), (0, 0)))
    result = offsets
    for tap_idx in range(KERNEL):
        result = result + kernel[tap_idx] * padded[:, tap_idx:tap_idx + LEN]
    return result.reshape(SEQS * LEN, FF)

def reference(tokens, norm_gain, gate_weight, up_weight, gate_taps, up_taps, gate_bias, up_bias, down_weight):
    carried = tokens.reshape(SEQS * LEN, D).astype(jnp.float32)
    for layer_idx in range(LAYERS):
        row_squares = lax.optimization_barrier(jnp.sum(carried * carried, axis=1))
        scaled = (carried * norm_gain[layer_idx]).astype(jnp.bfloat16)
        inverse = lax.rsqrt(row_squares / D + eps)
        gate_pre = (jnp.dot(scaled, gate_weight[layer_idx], preferred_element_type=jnp.float32) * inverse[:, None]).astype(jnp.bfloat16)
        up_pre = (jnp.dot(scaled, up_weight[layer_idx], preferred_element_type=jnp.float32) * inverse[:, None]).astype(jnp.bfloat16)
        gate_conv = causal_conv(gate_pre, gate_taps[layer_idx], gate_bias[layer_idx])
        up_conv = causal_conv(up_pre, up_taps[layer_idx], up_bias[layer_idx])
        hidden = (jax.nn.silu(gate_conv) * up_conv).astype(jnp.bfloat16)
        branch = jnp.dot(hidden, down_weight[layer_idx], preferred_element_type=jnp.float32)
        carried = resid_scale * carried + branch
    return carried.astype(jnp.bfloat16).reshape(SEQS, LEN, D)
```

```python
import functools

import jax
import jax.numpy as jnp
from jax import lax
from jax.experimental import pallas as pl
from jax.experimental.pallas import tpu as pltpu
from jax.sharding import PartitionSpec as P

EPS = 1e-06
RESID = 0.5
LANES = 128
CORES = 2
LAG_Y, LAG_Z, LAG_HY, LAG_HZ = 2, 2, 2, 2
TAIL_SUM, TAIL_END = 1, 4

MESH = pl.DeviceIdType.MESH
F32, BF16 = jnp.float32, jnp.bfloat16


def kernel(
    dims,
    tok_ref, gain_ref, gw_hbm, uw_hbm, gt_ref, ut_ref, gb_ref, ub_ref, dw_hbm,
    out_ref,
    gw_ref, uw_ref, dw_ref, carried, scaled, inv, acc,
    sq_own, sq_in, part, y_in, z_in, hid, c_out, c_in, c_sum,
    w_sem, sq_s, sq_r, y_s, y_r, z_s, z_r, hy_s, hy_r, hz_s, hz_r, c_s, c_r, ca_s, ca_r,
):
    n_ra, n_cb, nz, groups, rows, length, layers, width, chunks = dims
    ny = n_ra // nz
    blocks = width // LANES
    per_layer = groups * chunks
    half_rows = rows // CORES
    me_ra = lax.axis_index("ra")
    me_cb = lax.axis_index("cb")
    me_z, me_y = me_ra // ny, me_ra % ny
    core = me_cb % CORES
    seq, block = me_y // blocks, me_y % blocks

    def weight_copies(layer, i):
        cols = pl.ds(pl.multiple_of(i * width, width), width)
        return [
            pltpu.make_async_copy(
                gw_hbm.at[layer, :, cols], gw_ref.at[layer, :, cols], w_sem.at[layer, i, 0]
            ),
            pltpu.make_async_copy(
                uw_hbm.at[layer, :, cols], uw_ref.at[layer, :, cols], w_sem.at[layer, i, 1]
            ),
            pltpu.make_async_copy(
                dw_hbm.at[layer, cols], dw_ref.at[layer, cols], w_sem.at[layer, i, 2]
            ),
        ]

    for layer in range(layers):
        def fetch(i, _, layer=layer):
            for copy in weight_copies(layer, i):
                copy.start()
            return 0

        lax.fori_loop(0, chunks, fetch, 0)

    barrier = pltpu.get_barrier_semaphore()
    for step in range(1, n_ra):
        pl.semaphore_signal(
            barrier, inc=1, device_id={"ra": lax.rem(me_ra + step, n_ra)}, device_id_type=MESH
        )
    for step in range(1, n_cb):
        pl.semaphore_signal(
            barrier, inc=1, device_id={"cb": lax.rem(me_cb + step, n_cb)}, device_id_type=MESH
        )

    def remote(src, dst, send, recv, **where):
        return pltpu.make_async_remote_copy(
            src_ref=src, dst_ref=dst, send_sem=send, recv_sem=recv,
            device_id=where, device_id_type=MESH,
        )

    def square_copy(layer, g, step):
        return remote(
            sq_own.at[layer, g], sq_in.at[layer, g, step - 1],
            sq_s.at[layer, g, step - 1], sq_r.at[layer, g, step - 1],
            ra=lax.rem(me_ra + step, n_ra),
        )

    def y_copy(at, step):
        to = lax.rem(me_y + step, ny)
        return remote(
            part.at[at, to], y_in.at[at, step - 1],
            y_s.at[at, step - 1], y_r.at[at, step - 1], ra=me_z * ny + to,
        )

    def along(end):
        return lax.rem(me_z + 2 * end - 1 + nz, nz) * ny + me_y

    def z_copy(at, end):
        return remote(part.at[at, me_y], z_in.at[at], z_s.at[at], z_r.at[at], ra=along(end))

    def hy_copy(at, step, y):
        to = lax.rem(me_y + step, ny)
        block = hid.at[at, y]
        return remote(
            block, block, hy_s.at[at, step - 1], hy_r.at[at, step - 1], ra=me_z * ny + to
        )

    def hz_copy(at, end):
        return remote(hid.at[at], hid.at[at], hz_s.at[at], hz_r.at[at], ra=along(1 - end))

    def core_copy(layer, g):
        return remote(
            c_out.at[layer, g], c_in.at[layer, g], c_s.at[layer, g], c_r.at[layer, g],
            cb=me_cb + 1 - 2 * core,
        )

    def sum_copy(layer, g, step, block):
        to = lax.rem(me_cb + step, n_cb)
        block = c_sum.at[layer, g, block]
        return remote(
            block, block, ca_s.at[layer, g, step - 1], ca_r.at[layer, g, step - 1], cb=to
        )

    row_in_seq = lax.broadcasted_iota(jnp.int32, (length, LANES), 0)

    def prepare(layer, g):
        values = carried[g]
        squares = jnp.sum(values * values, axis=1, keepdims=True)
        sq_own[layer, g] = jnp.transpose(jnp.broadcast_to(squares, (rows, LANES)))[:1]
        scaled[g] = (values * gain_ref[layer]).astype(BF16)
        acc[g] = jnp.zeros(acc.shape[1:], F32)

    def send_squares(layer, g):
        for step in range(1, n_ra):
            square_copy(layer, g, step).start()

    def scale(layer, g):
        total = sq_own[layer, g]
        for step in range(1, n_ra):
            square_copy(layer, g, step).wait()
            total = total + sq_in[layer, g, step - 1]
        total = jnp.transpose(jnp.broadcast_to(total, (LANES, rows)))
        inv[g] = lax.rsqrt(total / (n_ra * gain_ref.shape[2]) + EPS)

    def project(layer, g, i, at):
        @pl.when(g == 0)
        def _():
            for copy in weight_copies(layer, i)[:2]:
                copy.wait()

        cols = pl.ds(pl.multiple_of(i * width, width), width)
        for half, w_ref in enumerate((gw_ref, uw_ref)):
            product = jnp.dot(scaled[g], w_ref[layer, :, cols], preferred_element_type=F32)
            for unit in range(ny):
                s, b = unit // blocks, unit % blocks
                part[at, unit, :, half * LANES:(half + 1) * LANES] = product[
                    s * length:(s + 1) * length, b * LANES:(b + 1) * LANES
                ].astype(BF16)
        for step in range(1, ny):
            y_copy(at, step).start()

    def add_y(at):
        value = part[at, me_y].astype(F32)
        for step in range(1, ny):
            y_copy(at, step).wait_recv()
            value = value + y_in[at, step - 1].astype(F32)
        part[at, me_y] = value.astype(BF16)

    def add_z(at, end):
        z_copy(at, end).wait_recv()
        return part[at, me_y].astype(F32) + z_in[at].astype(F32)

    def activate(layer, g, i, at, end):
        value = add_z(at, end)
        cols = pl.ds(pl.multiple_of(i * width + block * LANES, LANES), LANES)
        factor = inv[g, pl.ds(pl.multiple_of(seq * length, length), length), :]
        conv = []
        for half, (taps, bias) in enumerate(((gt_ref, gb_ref), (ut_ref, ub_ref))):
            pre = value[:, half * LANES:(half + 1) * LANES] * factor
            pre = pre.astype(BF16).astype(F32)
            last = jnp.where(row_in_seq >= 1, pltpu.roll(pre, 1, 0), 0.0)
            older = jnp.where(row_in_seq >= 2, pltpu.roll(pre, 2, 0), 0.0)
            tap = [taps[layer, pl.ds(k, 1), cols] for k in range(3)]
            conv.append(
                bias[layer, :, cols] + tap[0] * older + tap[1] * last + tap[2] * pre
            )
        gate, up = conv
        hid[at, me_y] = (gate / (1.0 + jnp.exp(-gate)) * up).astype(BF16)
        for step in range(1, ny):
            hy_copy(at, step, me_y).start()

    def gather_y(at):
        for step in range(1, ny):
            hy_copy(at, step, lax.rem(me_y - step + ny, ny)).wait_recv()

    def down(layer, g, i, at):
        @pl.when(g == 0)
        def _():
            weight_copies(layer, i)[2].wait()

        depth = pl.ds(pl.multiple_of(i * width, width), width)
        units = [hid[at, unit] for unit in range(ny)]
        hidden = jnp.concatenate(
            [jnp.concatenate(units[s:s + blocks], axis=1) for s in range(0, ny, blocks)], axis=0
        )
        acc[g] += jnp.dot(hidden, dw_ref[layer, depth, :], preferred_element_type=F32)

    def settle(at, end, hop):
        for step in range(1, ny):
            y_copy(at, step).wait_send()

        @pl.when(hop < nz - 1)
        def _():
            z_copy(at, end).wait_send()

        @pl.when(hop == nz - 1)
        def _():
            for step in range(1, ny):
                hy_copy(at, step, me_y).wait_send()

        @pl.when(hop > 0)
        def _():
            hz_copy(at, end).wait_send()

    def half_of(which):
        return pl.ds(pl.multiple_of(which * half_rows, half_rows), half_rows)

    def core_sum(layer, g):
        c_out[layer, g] = acc[g, half_of(1 - core), :].astype(BF16)
        core_copy(layer, g).start()

    def chip_sum(layer, g):
        core_copy(layer, g).wait()
        value = acc[g, half_of(core), :] + c_in[layer, g].astype(F32)
        c_sum[layer, g, me_cb] = value.astype(BF16)
        for step in range(1, n_cb):
            sum_copy(layer, g, step, me_cb).start()

    def finish(layer, g):
        for step in range(1, n_cb):
            sum_copy(layer, g, step, lax.rem(me_cb - step + n_cb, n_cb)).wait_recv()
            sum_copy(layer, g, step, me_cb).wait_send()
        for c in range(CORES):
            branch = c_sum[layer, g, c].astype(F32)
            for chip in range(1, n_cb // CORES):
                branch = branch + c_sum[layer, g, chip * CORES + c].astype(F32)
            span = pl.ds(c * half_rows, half_rows)
            carried[g, span, :] = RESID * carried[g, span, :] + branch

        @pl.when(layer < layers - 1)
        def _():
            prepare(layer + 1, g)
            send_squares(layer + 1, g)

        @pl.when(layer == layers - 1)
        def _():
            out_ref[g] = carried[g].astype(out_ref.dtype)

    for g in range(groups):
        carried[g] = tok_ref[g].astype(F32)
        prepare(0, g)
    pl.semaphore_wait(barrier, n_ra + n_cb - 2)
    for g in range(groups):
        send_squares(0, g)

    act_lag = LAG_Y + LAG_Z * (nz - 1)
    gather_lag = act_lag + LAG_HY
    down_lag = gather_lag + LAG_HZ * (nz - 1)
    total_lag = down_lag + TAIL_END
    stride = max(per_layer, chunks + total_lag)

    def body(t, _):
        def place(lag):
            at = t - lag
            layer, q = lax.div(at, stride), lax.rem(at, stride)
            active = (at >= 0) & (q < per_layer) & (layer < layers)
            end = lax.rem(q, 2)
            hop = jnp.where(end == 0, nz - 1 - me_z, me_z)
            return active, layer, lax.div(q, chunks), lax.rem(q, chunks), layer * per_layer + q, end, hop

        active, layer, g, i, at, end, hop = place(down_lag + TAIL_END)

        @pl.when(active & (i == chunks - 1))
        def _():
            finish(layer, g)

        active, layer, g, i, at, end, hop = place(down_lag + TAIL_SUM)

        @pl.when(active & (i == chunks - 1))
        def _():
            chip_sum(layer, g)

        for far in range(nz - 2, 0, -1):
            active, layer, g, i, at, end, hop = place(gather_lag + LAG_HZ * far)

            @pl.when(active & (hop == nz - 1 - far))
            def _():
                hz_copy(at, end).wait_recv()
                hz_copy(at, end).start()

        active, layer, g, i, at, end, hop = place(gather_lag)

        @pl.when(active & (hop == nz - 1))
        def _():
            gather_y(at)
            hz_copy(at, end).start()

        active, layer, g, i, at, end, hop = place(act_lag)

        @pl.when(active & (i == 0))
        def _():
            scale(layer, g)

        @pl.when(active & (hop == nz - 1))
        def _():
            activate(layer, g, i, at, end)

        for k in range(nz - 2, 0, -1):
            active, layer, g, i, at, end, hop = place(LAG_Y + LAG_Z * k)

            @pl.when(active & (hop == k))
            def _():
                part[at, me_y] = add_z(at, end).astype(BF16)
                z_copy(at, end).start()

        active, layer, g, i, at, end, hop = place(LAG_Y)

        @pl.when(active)
        def _():
            add_y(at)

        @pl.when(active & (hop == 0))
        def _():
            z_copy(at, end).start()

        active, layer, g, i, at, end, hop = place(0)

        @pl.when(active)
        def _():
            project(layer, g, i, at)

        active, layer, g, i, at, end, hop = place(down_lag)

        @pl.when(active & (hop == 0))
        def _():
            hz_copy(at, end).wait_recv()

        @pl.when(active)
        def _():
            down(layer, g, i, at)
            settle(at, end, hop)

        @pl.when(active & (i == chunks - 1))
        def _():
            core_sum(layer, g)

        return 0

    lax.fori_loop(0, stride * (layers - 1) + per_layer + total_lag, body, 0)


def per_device(n_ra, n_cb, tokens, gain, gw, uw, gt, ut, gb, ub, dw):
    seqs, length, d = tokens.shape
    layers, _, ff = gw.shape
    nz = seqs
    ny = n_ra // nz
    blocks = ny if ff % (ny * LANES) == 0 else 1
    width = blocks * LANES
    groups = seqs * blocks // ny
    rows = seqs * length // groups
    chunks = ff // width
    n = layers * groups * chunks
    dims = (n_ra, n_cb, nz, groups, rows, length, layers, width, chunks)
    vmem = pl.BlockSpec(memory_space=pltpu.VMEM)
    hbm = pl.BlockSpec(memory_space=pl.ANY)
    dma = pltpu.SemaphoreType.DMA
    ys = max(ny - 1, 1)
    half = rows // CORES
    scratch = [
        pltpu.VMEM((layers, d, ff), BF16),
        pltpu.VMEM((layers, d, ff), BF16),
        pltpu.VMEM((layers, ff, d), BF16),
        pltpu.VMEM((groups, rows, d), F32),
        pltpu.VMEM((groups, rows, d), BF16),
        pltpu.VMEM((groups, rows, LANES), F32),
        pltpu.VMEM((groups, rows, d), F32),
        pltpu.VMEM((layers, groups, 1, rows), F32),
        pltpu.VMEM((layers, groups, n_ra - 1, 1, rows), F32),
        pltpu.VMEM((n, ny, length, 2 * LANES), BF16),
        pltpu.VMEM((n, ys, length, 2 * LANES), BF16),
        pltpu.VMEM((n, length, 2 * LANES), BF16),
        pltpu.VMEM((n, ny, length, LANES), BF16),
        pltpu.VMEM((layers, groups, half, d), BF16),
        pltpu.VMEM((layers, groups, half, d), BF16),
        pltpu.VMEM((layers, groups, n_cb, half, d), BF16),
        dma((layers, chunks, 3)),
        dma((layers, groups, n_ra - 1)), dma((layers, groups, n_ra - 1)),
        dma((n, ys)), dma((n, ys)),
        dma((n,)), dma((n,)),
        dma((n, ys)), dma((n, ys)),
        dma((n,)), dma((n,)),
        dma((layers, groups)), dma((layers, groups)),
        dma((layers, groups, n_cb - 1)), dma((layers, groups, n_cb - 1)),
    ]
    out = pl.pallas_call(
        functools.partial(kernel, dims),
        out_shape=jax.ShapeDtypeStruct((groups, rows, d), tokens.dtype),
        in_specs=[vmem, vmem, hbm, hbm, vmem, vmem, vmem, vmem, hbm],
        out_specs=vmem,
        scratch_shapes=scratch,
        compiler_params=pltpu.CompilerParams(
            collective_id=0, has_side_effects=True, vmem_limit_bytes=60 * 1024 * 1024
        ),
        name="blocks",
    )(
        tokens.reshape(groups, rows, d), gain[:, None, :], gw, uw, gt, ut,
        gb[:, None, :], ub[:, None, :], dw,
    )
    return out.reshape(tokens.shape)


def solution(mesh):
    in_specs = (
        P(None, None, "ra"),
        P(None, "ra"),
        P(None, "ra", "cb"),
        P(None, "ra", "cb"),
        P(None, None, "cb"),
        P(None, None, "cb"),
        P(None, "cb"),
        P(None, "cb"),
        P(None, "cb", "ra"),
    )
    return jax.shard_map(
        functools.partial(per_device, mesh.shape["ra"], mesh.shape["cb"]),
        mesh=mesh, in_specs=in_specs, out_specs=P(None, None, "ra"), check_vma=False,
    )
```

```python
import functools

import jax
import jax.numpy as jnp
from jax import lax
from jax.experimental import pallas as pl
from jax.experimental.pallas import tpu as pltpu
from jax.sharding import PartitionSpec as P

EPS = 1e-06
RESID = 0.5
LANES = 128
CORES = 2
LAG_Y, LAG_Z, LAG_HY, LAG_HZ = 4, 4, 4, 4
TAIL_CHIP, TAIL_SUM, TAIL_END = 1, 4, 5
SPLIT, SPREAD = 1 / 2, 1 / 2

MESH = pl.DeviceIdType.MESH
F32, BF16 = jnp.float32, jnp.bfloat16


def kernel(
    dims,
    tok_ref, gain_ref, gw_hbm, uw_hbm, gt_ref, ut_ref, gb_ref, ub_ref, dw_hbm,
    out_ref,
    gw_ref, uw_ref, dw_ref, carried, scaled, inv, acc,
    sq_own, sq_in, part, y_in, z_in, hid, c_out, c_in, c_sum, c_all,
    w_sem, sq_s, sq_r, y_s, y_r, z_s, z_r, wz_s, wz_r, wy_s, wy_r, hy_s, hy_r, hz_s, hz_r, nz_s, nz_r, ny_s, ny_r, c_s, c_r, cs_s, cs_r, ca_s, ca_r,
):
    n_ra, n_cb, nz, groups, rows, length, layers, width, chunks = dims
    ny = n_ra // nz
    blocks = width // LANES
    per_layer = groups * chunks
    half_rows = rows // CORES
    me_ra = lax.axis_index("ra")
    me_cb = lax.axis_index("cb")
    me_z, me_y = me_ra // ny, me_ra % ny
    core, chip, chips = me_cb % CORES, me_cb // CORES, n_cb // CORES
    seq, block = me_y // blocks, me_y % blocks

    def weight_copies(layer, i):
        cols = pl.ds(pl.multiple_of(i * width, width), width)
        return [
            pltpu.make_async_copy(
                gw_hbm.at[layer, :, cols], gw_ref.at[layer, :, cols], w_sem.at[layer, i, 0]
            ),
            pltpu.make_async_copy(
                uw_hbm.at[layer, :, cols], uw_ref.at[layer, :, cols], w_sem.at[layer, i, 1]
            ),
            pltpu.make_async_copy(
                dw_hbm.at[layer, cols], dw_ref.at[layer, cols], w_sem.at[layer, i, 2]
            ),
        ]

    for layer in range(layers):
        def fetch(i, _, layer=layer):
            for copy in weight_copies(layer, i):
                copy.start()
            return 0

        lax.fori_loop(0, chunks, fetch, 0)

    barrier = pltpu.get_barrier_semaphore()
    for step in range(1, n_ra):
        pl.semaphore_signal(
            barrier, inc=1, device_id={"ra": lax.rem(me_ra + step, n_ra)}, device_id_type=MESH
        )
    for step in range(1, n_cb):
        pl.semaphore_signal(
            barrier, inc=1, device_id={"cb": lax.rem(me_cb + step, n_cb)}, device_id_type=MESH
        )

    def remote(src, dst, send, recv, **where):
        return pltpu.make_async_remote_copy(
            src_ref=src, dst_ref=dst, send_sem=send, recv_sem=recv,
            device_id=where, device_id_type=MESH,
        )

    def square_copy(layer, g, step):
        return remote(
            sq_own.at[layer, g], sq_in.at[layer, g, step - 1],
            sq_s.at[layer, g, step - 1], sq_r.at[layer, g, step - 1],
            ra=lax.rem(me_ra + step, n_ra),
        )

    split = int(length * SPLIT) // 16 * 16
    first, rest = pl.ds(0, split), pl.ds(split, length - split)

    def y_copy(at, step):
        to = lax.rem(me_y + step, ny)
        return remote(
            part.at[at, to, first], y_in.at[at, step - 1, first],
            y_s.at[at, step - 1], y_r.at[at, step - 1], ra=me_z * ny + to,
        )

    def late_copy(at, step):
        to = lax.rem(me_y + step, ny)
        return remote(
            part.at[at, to, rest], y_in.at[at, step - 1, rest],
            wy_s.at[at, step - 1], wy_r.at[at, step - 1], ra=me_z * ny + to,
        )

    def along(end):
        return lax.rem(me_z + 2 * end - 1 + nz, nz) * ny + me_y

    def z_copy(at, end):
        return remote(
            part.at[at, me_y, first], z_in.at[at, 0, first], z_s.at[at], z_r.at[at],
            ra=along(end),
        )

    def wide_copy(at, end):
        return remote(
            part.at[at, :, rest], z_in.at[at, :, rest], wz_s.at[at], wz_r.at[at], ra=along(end)
        )

    def hy_copy(at, step, y):
        to = lax.rem(me_y + step, ny)
        block = hid.at[at, y]
        return remote(
            block, block, hy_s.at[at, step - 1], hy_r.at[at, step - 1], ra=me_z * ny + to
        )

    spread = int(length * SPREAD) // 16 * 16
    both, own = pl.ds(0, spread), pl.ds(spread, length - spread)

    def hz_copy(at, end):
        rows_of = hid.at[at, :, both]
        return remote(rows_of, rows_of, hz_s.at[at], hz_r.at[at], ra=along(1 - end))

    def own_copy(at, end):
        rows_of = hid.at[at, me_y, own]
        return remote(rows_of, rows_of, nz_s.at[at], nz_r.at[at], ra=along(1 - end))

    def cross_copy(at, step, y):
        rows_of = hid.at[at, y, own]
        return remote(
            rows_of, rows_of, ny_s.at[at, step - 1], ny_r.at[at, step - 1],
            ra=me_z * ny + lax.rem(me_y + step, ny),
        )

    def core_copy(layer, g):
        return remote(
            c_out.at[layer, g], c_in.at[layer, g], c_s.at[layer, g], c_r.at[layer, g],
            cb=me_cb + 1 - 2 * core,
        )

    def sum_copy(layer, g, step, source):
        piece = c_sum.at[layer, g, source]
        return remote(
            piece, piece, cs_s.at[layer, g, step - 1], cs_r.at[layer, g, step - 1],
            cb=lax.rem(chip + step, chips) * CORES + core,
        )

    def all_copy(layer, g, source):
        piece = c_all.at[layer, g, source]
        return remote(
            piece, piece, ca_s.at[layer, g], ca_r.at[layer, g], cb=me_cb + 1 - 2 * core
        )

    row_in_seq = lax.broadcasted_iota(jnp.int32, (length, LANES), 0)

    def of_layer(values, layer):
        picked = values[:1]
        for other in range(1, layers):
            picked = jnp.where(layer == other, values[other:other + 1], picked)
        return picked

    def prepare(layer, g):
        values = carried[g]
        squares = jnp.sum(values * values, axis=1, keepdims=True)
        sq_own[layer, g] = jnp.transpose(jnp.broadcast_to(squares, (rows, LANES)))[:1]
        scaled[g] = (values * of_layer(gain_ref[...], layer)).astype(BF16)
        acc[g] = jnp.zeros(acc.shape[1:], F32)

    def send_squares(layer, g):
        for step in range(1, n_ra):
            square_copy(layer, g, step).start()

    def scale(layer, g):
        total = sq_own[layer, g]
        for step in range(1, n_ra):
            square_copy(layer, g, step).wait()
            total = total + sq_in[layer, g, step - 1]
        total = jnp.transpose(jnp.broadcast_to(total, (LANES, rows)))
        inv[g] = lax.rsqrt(total / (n_ra * gain_ref.shape[1]) + EPS)

    def project(layer, g, i, at, end, hop):
        @pl.when(g == 0)
        def _():
            for copy in weight_copies(layer, i)[:2]:
                copy.wait()

        cols = pl.ds(pl.multiple_of(i * width, width), width)
        for half, w_ref in enumerate((gw_ref, uw_ref)):
            product = jnp.dot(scaled[g], w_ref[layer, :, cols], preferred_element_type=F32)
            for unit in range(ny):
                s, b = unit // blocks, unit % blocks
                part[at, unit, :, half * LANES:(half + 1) * LANES] = product[
                    s * length:(s + 1) * length, b * LANES:(b + 1) * LANES
                ].astype(BF16)

        for step in range(1, ny):
            y_copy(at, step).start()

        @pl.when(hop == 0)
        def _():
            wide_copy(at, end).start()

    def add_y(at, copy, span):
        value = part[at, me_y, span].astype(F32)
        for step in range(1, ny):
            copy(at, step).wait_recv()
            value = value + y_in[at, step - 1, span].astype(F32)
        return value

    def add_z(at, end):
        z_copy(at, end).wait_recv()
        return part[at, me_y, first].astype(F32) + z_in[at, 0, first].astype(F32)

    def add_wide(at, end):
        wide_copy(at, end).wait_recv()
        for unit in range(ny):
            total = part[at, unit, rest].astype(F32) + z_in[at, unit, rest].astype(F32)
            part[at, unit, rest] = total.astype(BF16)

    def activate(layer, g, i, at, end):
        value = jnp.concatenate([add_z(at, end), add_y(at, late_copy, rest)], axis=0)
        cols = pl.ds(pl.multiple_of(i * width + block * LANES, LANES), LANES)
        factor = inv[g, pl.ds(pl.multiple_of(seq * length, length), length), :]
        conv = []
        for half, (taps, bias) in enumerate(((gt_ref, gb_ref), (ut_ref, ub_ref))):
            pre = value[:, half * LANES:(half + 1) * LANES] * factor
            pre = pre.astype(BF16).astype(F32)
            last = jnp.where(row_in_seq >= 1, pltpu.roll(pre, 1, 0), 0.0)
            older = jnp.where(row_in_seq >= 2, pltpu.roll(pre, 2, 0), 0.0)
            tap = [of_layer(taps[k, :, cols], layer) for k in range(3)]
            conv.append(
                of_layer(bias[:, cols], layer) + tap[0] * older + tap[1] * last + tap[2] * pre
            )
        gate, up = conv
        hid[at, me_y] = (gate / (1.0 + jnp.exp(-gate)) * up).astype(BF16)
        for step in range(1, ny):
            hy_copy(at, step, me_y).start()
        own_copy(at, end).start()

    def gather_y(at):
        for step in range(1, ny):
            hy_copy(at, step, lax.rem(me_y - step + ny, ny)).wait_recv()

    def down(layer, g, i, at):
        @pl.when(g == 0)
        def _():
            weight_copies(layer, i)[2].wait()

        depth = pl.ds(pl.multiple_of(i * width, width), width)
        units = [hid[at, unit] for unit in range(ny)]
        hidden = jnp.concatenate(
            [jnp.concatenate(units[s:s + blocks], axis=1) for s in range(0, ny, blocks)], axis=0
        )
        acc[g] += jnp.dot(hidden, dw_ref[layer, depth, :], preferred_element_type=F32)

    def settle(at, end, hop):
        for step in range(1, ny):
            y_copy(at, step).wait_send()

        @pl.when(hop < nz - 1)
        def _():
            z_copy(at, end).wait_send()
            wide_copy(at, end).wait_send()

        @pl.when(hop == nz - 1)
        def _():
            for step in range(1, ny):
                late_copy(at, step).wait_send()
                hy_copy(at, step, me_y).wait_send()

        @pl.when(hop > 0)
        def _():
            hz_copy(at, end).wait_send()
            own_copy(at, end).wait_send()

        @pl.when(hop < nz - 1)
        def _():
            for step in range(1, ny):
                cross_copy(at, step, me_y).wait_send()

    def half_of(which):
        return pl.ds(pl.multiple_of(which * half_rows, half_rows), half_rows)

    def core_sum(layer, g):
        c_out[layer, g] = acc[g, half_of(1 - core), :].astype(BF16)
        core_copy(layer, g).start()

    def chip_sum(layer, g):
        core_copy(layer, g).wait()
        value = acc[g, half_of(core), :] + c_in[layer, g].astype(F32)
        c_sum[layer, g, chip] = value.astype(BF16)
        for step in range(1, chips):
            sum_copy(layer, g, step, chip).start()

    def total_sum(layer, g):
        for step in range(1, chips):
            sum_copy(layer, g, step, lax.rem(chip - step + chips, chips)).wait_recv()
            sum_copy(layer, g, step, chip).wait_send()
        value = c_sum[layer, g, 0].astype(F32)
        for other in range(1, chips):
            value = value + c_sum[layer, g, other].astype(F32)
        c_all[layer, g, core] = value.astype(BF16)
        all_copy(layer, g, core).start()

    def finish(layer, g):
        all_copy(layer, g, 1 - core).wait_recv()
        all_copy(layer, g, core).wait_send()
        branch = c_all[layer, g].reshape(rows, c_all.shape[4]).astype(F32)
        carried[g] = RESID * carried[g] + branch

        @pl.when(layer < layers - 1)
        def _():
            prepare(layer + 1, g)
            send_squares(layer + 1, g)

        @pl.when(layer == layers - 1)
        def _():
            out_ref[g] = carried[g].astype(out_ref.dtype)

    def enter(g):
        carried[g] = tok_ref[g].astype(F32)
        prepare(0, g)

    enter(0)
    pl.semaphore_wait(barrier, n_ra + n_cb - 2)
    send_squares(0, 0)

    act_lag = LAG_Y + LAG_Z * (nz - 1)
    gather_lag = act_lag + LAG_HY
    down_lag = gather_lag + LAG_HZ * (nz - 1)
    total_lag = down_lag + TAIL_END
    stride = max(per_layer, chunks + total_lag)

    def body(t, _):
        def place(lag):
            at = t - lag
            layer, q = lax.div(at, stride), lax.rem(at, stride)
            active = (at >= 0) & (q < per_layer) & (layer < layers)
            end = lax.rem(q, 2)
            hop = jnp.where(end == 0, nz - 1 - me_z, me_z)
            spot = lax.div(q, chunks), lax.rem(q, chunks), layer * per_layer + q
            return active, layer, *spot, end, hop

        for lag, stage in ((TAIL_END, finish), (TAIL_SUM, total_sum), (TAIL_CHIP, chip_sum)):
            active, layer, g, i, at, end, hop = place(down_lag + lag)

            @pl.when(active & (i == chunks - 1))
            def _():
                stage(layer, g)

        for far in range(nz - 1, 0, -1):
            active, layer, g, i, at, end, hop = place(act_lag + LAG_HZ * far)

            @pl.when(active & (hop == nz - 1 - far))
            def _():
                own_copy(at, end).wait_recv()
                if far < nz - 1:
                    own_copy(at, end).start()
                for step in range(1, ny):
                    cross_copy(at, step, me_y).start()

        for far in range(nz - 2, 0, -1):
            active, layer, g, i, at, end, hop = place(gather_lag + LAG_HZ * far)

            @pl.when(active & (hop == nz - 1 - far))
            def _():
                hz_copy(at, end).wait_recv()
                hz_copy(at, end).start()

        active, layer, g, i, at, end, hop = place(gather_lag)

        @pl.when(active & (hop == nz - 1))
        def _():
            gather_y(at)
            hz_copy(at, end).start()

        active, layer, g, i, at, end, hop = place(act_lag)

        @pl.when(active & (i == 0))
        def _():
            scale(layer, g)

        @pl.when(active & (hop == nz - 1))
        def _():
            activate(layer, g, i, at, end)

        active, layer, g, i, at, end, hop = place(LAG_Z * (nz - 1))

        @pl.when(active & (hop == nz - 1))
        def _():
            add_wide(at, end)
            for step in range(1, ny):
                late_copy(at, step).start()

        for k in range(nz - 2, 0, -1):
            active, layer, g, i, at, end, hop = place(LAG_Z * k)

            @pl.when(active & (hop == k))
            def _():
                add_wide(at, end)
                wide_copy(at, end).start()

            active, layer, g, i, at, end, hop = place(LAG_Y + LAG_Z * k)

            @pl.when(active & (hop == k))
            def _():
                part[at, me_y, first] = add_z(at, end).astype(BF16)
                z_copy(at, end).start()

        active, layer, g, i, at, end, hop = place(LAG_Y)

        @pl.when(active)
        def _():
            part[at, me_y, first] = add_y(at, y_copy, first).astype(BF16)

        @pl.when(active & (hop == 0))
        def _():
            z_copy(at, end).start()

        active, layer, g, i, at, end, hop = place(0)

        @pl.when(active & (layer == 0) & (i == 0) & (g > 0))
        def _():
            enter(g)
            send_squares(0, g)

        @pl.when(active)
        def _():
            project(layer, g, i, at, end, hop)

        active, layer, g, i, at, end, hop = place(down_lag)

        @pl.when(active & (hop == 0))
        def _():
            hz_copy(at, end).wait_recv()

        @pl.when(active & (hop < nz - 1))
        def _():
            for step in range(1, ny):
                cross_copy(at, step, lax.rem(me_y - step + ny, ny)).wait_recv()

        @pl.when(active)
        def _():
            down(layer, g, i, at)
            settle(at, end, hop)

        @pl.when(active & (i == chunks - 1))
        def _():
            core_sum(layer, g)

        return 0

    lax.fori_loop(0, stride * (layers - 1) + per_layer + total_lag, body, 0)


def per_device(n_ra, n_cb, tokens, gain, gw, uw, gt, ut, gb, ub, dw):
    seqs, length, d = tokens.shape
    layers, _, ff = gw.shape
    nz = seqs
    ny = n_ra // nz
    blocks = ny if ff % (ny * LANES) == 0 else 1
    width = blocks * LANES
    groups = seqs * blocks // ny
    rows = seqs * length // groups
    chunks = ff // width
    n = layers * groups * chunks
    dims = (n_ra, n_cb, nz, groups, rows, length, layers, width, chunks)
    vmem = pl.BlockSpec(memory_space=pltpu.VMEM)
    hbm = pl.BlockSpec(memory_space=pl.ANY)
    dma = pltpu.SemaphoreType.DMA
    ys = max(ny - 1, 1)
    half, chips = rows // CORES, n_cb // CORES
    scratch = [
        pltpu.VMEM((layers, d, ff), BF16),
        pltpu.VMEM((layers, d, ff), BF16),
        pltpu.VMEM((layers, ff, d), BF16),
        pltpu.VMEM((groups, rows, d), F32),
        pltpu.VMEM((groups, rows, d), BF16),
        pltpu.VMEM((groups, rows, LANES), F32),
        pltpu.VMEM((groups, rows, d), F32),
        pltpu.VMEM((layers, groups, 1, rows), F32),
        pltpu.VMEM((layers, groups, n_ra - 1, 1, rows), F32),
        pltpu.VMEM((n, ny, length, 2 * LANES), BF16),
        pltpu.VMEM((n, ys, length, 2 * LANES), BF16),
        pltpu.VMEM((n, ny, length, 2 * LANES), BF16),
        pltpu.VMEM((n, ny, length, LANES), BF16),
        pltpu.VMEM((layers, groups, half, d), BF16),
        pltpu.VMEM((layers, groups, half, d), BF16),
        pltpu.VMEM((layers, groups, chips, half, d), BF16),
        pltpu.VMEM((layers, groups, CORES, half, d), BF16),
        dma((layers, chunks, 3)),
        dma((layers, groups, n_ra - 1)), dma((layers, groups, n_ra - 1)),
        dma((n, ys)), dma((n, ys)),
        dma((n,)), dma((n,)),
        dma((n,)), dma((n,)),
        dma((n, ys)), dma((n, ys)),
        dma((n, ys)), dma((n, ys)),
        dma((n,)), dma((n,)),
        dma((n,)), dma((n,)),
        dma((n, ys)), dma((n, ys)),
        dma((layers, groups)), dma((layers, groups)),
        dma((layers, groups, max(chips - 1, 1))), dma((layers, groups, max(chips - 1, 1))),
        dma((layers, groups)), dma((layers, groups)),
    ]
    out = pl.pallas_call(
        functools.partial(kernel, dims),
        out_shape=jax.ShapeDtypeStruct((groups, rows, d), tokens.dtype),
        in_specs=[vmem, vmem, hbm, hbm, vmem, vmem, vmem, vmem, hbm],
        out_specs=vmem,
        scratch_shapes=scratch,
        compiler_params=pltpu.CompilerParams(
            collective_id=0, has_side_effects=True, vmem_limit_bytes=60 * 1024 * 1024
        ),
        name="blocks",
    )(
        tokens.reshape(groups, rows, d), gain, gw, uw,
        jnp.transpose(gt, (1, 0, 2)), jnp.transpose(ut, (1, 0, 2)), gb, ub, dw,
    )
    return out.reshape(tokens.shape)


def solution(mesh):
    in_specs = (
        P(None, None, "ra"),
        P(None, "ra"),
        P(None, "ra", "cb"),
        P(None, "ra", "cb"),
        P(None, None, "cb"),
        P(None, None, "cb"),
        P(None, "cb"),
        P(None, "cb"),
        P(None, "cb", "ra"),
    )
    return jax.shard_map(
        functools.partial(per_device, mesh.shape["ra"], mesh.shape["cb"]),
        mesh=mesh, in_specs=in_specs, out_specs=P(None, None, "ra"), check_vma=False,
    )
```

```python
import functools

import jax
import jax.numpy as jnp
from jax import lax
from jax.experimental import pallas as pl
from jax.experimental.pallas import tpu as pltpu
from jax.sharding import PartitionSpec as P

EPS = 1e-06
RESID = 0.5
LANES = 128
CORES = 2
LAG_Y, LAG_Z, LAG_HY, LAG_HZ = 4, 4, 4, 4
TAIL_CHIP, TAIL_SUM, TAIL_END = 1, 4, 5
SPLIT, SPREAD = 1 / 2, 1 / 2

MESH = pl.DeviceIdType.MESH
F32, BF16 = jnp.float32, jnp.bfloat16


def kernel(
    dims,
    tok_hbm, gain_hbm, gw_hbm, uw_hbm, gt_hbm, ut_hbm, gb_hbm, ub_hbm, dw_hbm,
    out_ref,
    tok_ref, gain_ref, gt_ref, ut_ref, gb_ref, ub_ref,
    gw_ref, uw_ref, dw_ref, carried, scaled, inv, acc,
    sq_own, sq_y, sq_sum, sq_fwd, sq_z, part, y_in, z_in, hid, c_out, c_in, c_sum, c_all,
    i_sem, w_sem, sq_s, sq_r, sz_s, sz_r, y_s, y_r, z_s, z_r, wz_s, wz_r, wy_s, wy_r, hy_s, hy_r, hz_s, hz_r, nz_s, nz_r, ny_s, ny_r, c_s, c_r, cs_s, cs_r, ca_s, ca_r,
):
    n_ra, n_cb, nz, groups, rows, length, layers, width, chunks = dims
    ny = n_ra // nz
    blocks = width // LANES
    per_layer = groups * chunks
    half_rows = rows // CORES
    me_ra = lax.axis_index("ra")
    me_cb = lax.axis_index("cb")
    me_z, me_y = me_ra // ny, me_ra % ny
    core, chip, chips = me_cb % CORES, me_cb // CORES, n_cb // CORES
    seq, block = me_y // blocks, me_y % blocks

    def weight_copies(layer, i):
        cols = pl.ds(pl.multiple_of(i * width, width), width)
        return [
            pltpu.make_async_copy(
                gw_hbm.at[layer, :, cols], gw_ref.at[layer, :, cols], w_sem.at[layer, i, 0]
            ),
            pltpu.make_async_copy(
                uw_hbm.at[layer, :, cols], uw_ref.at[layer, :, cols], w_sem.at[layer, i, 1]
            ),
            pltpu.make_async_copy(
                dw_hbm.at[layer, cols], dw_ref.at[layer, cols], w_sem.at[layer, i, 2]
            ),
        ]

    barrier = pltpu.get_barrier_semaphore()
    def greet(**where):
        pl.semaphore_signal(barrier, inc=1, device_id=where, device_id_type=MESH)

    for step in range(1, ny):
        greet(ra=me_z * ny + lax.rem(me_y + step, ny))
    for step in range(1, chips):
        greet(cb=lax.rem(chip + step, chips) * CORES + core)
    greet(cb=me_cb + 1 - 2 * core)

    @pl.when(me_z > 0)
    def _():
        greet(ra=me_ra - ny)

    @pl.when(me_z < nz - 1)
    def _():
        greet(ra=me_ra + ny)

    guests = ny + chips - 1 + jnp.where(me_z > 0, 1, 0) + jnp.where(me_z < nz - 1, 1, 0)

    inputs = [
        pltpu.make_async_copy(source, target, i_sem.at[k])
        for k, (source, target) in enumerate((
            (tok_hbm, tok_ref), (gain_hbm, gain_ref), (gt_hbm, gt_ref), (ut_hbm, ut_ref),
            (gb_hbm, gb_ref), (ub_hbm, ub_ref),
        ))
    ]
    for copy in inputs:
        copy.start()

    for layer in range(layers):
        def fetch(i, _, layer=layer):
            for copy in weight_copies(layer, i):
                copy.start()
            return 0

        lax.fori_loop(0, chunks, fetch, 0)

    def remote(src, dst, send, recv, **where):
        return pltpu.make_async_remote_copy(
            src_ref=src, dst_ref=dst, send_sem=send, recv_sem=recv,
            device_id=where, device_id_type=MESH,
        )

    def square_copy(layer, g, step):
        return remote(
            sq_own.at[layer, g], sq_y.at[layer, g, step - 1],
            sq_s.at[layer, g, step - 1], sq_r.at[layer, g, step - 1],
            ra=me_z * ny + lax.rem(me_y + step, ny),
        )

    def square_along(layer, g, end):
        return remote(
            sq_fwd.at[layer, g, end], sq_z.at[layer, g, end],
            sz_s.at[layer, g, end], sz_r.at[layer, g, end], ra=along(end),
        )

    split = int(length * SPLIT) // 16 * 16
    first, rest = pl.ds(0, split), pl.ds(split, length - split)

    def y_copy(at, step):
        to = lax.rem(me_y + step, ny)
        return remote(
            part.at[at, to, first], y_in.at[at, step - 1, first],
            y_s.at[at, step - 1], y_r.at[at, step - 1], ra=me_z * ny + to,
        )

    def late_copy(at, step):
        to = lax.rem(me_y + step, ny)
        return remote(
            part.at[at, to, rest], y_in.at[at, step - 1, rest],
            wy_s.at[at, step - 1], wy_r.at[at, step - 1], ra=me_z * ny + to,
        )

    def along(end):
        return lax.rem(me_z + 2 * end - 1 + nz, nz) * ny + me_y

    def z_copy(at, end):
        return remote(
            part.at[at, me_y, first], z_in.at[at, 0, first], z_s.at[at], z_r.at[at],
            ra=along(end),
        )

    def wide_copy(at, end):
        return remote(
            part.at[at, :, rest], z_in.at[at, :, rest], wz_s.at[at], wz_r.at[at], ra=along(end)
        )

    def hy_copy(at, step, y):
        to = lax.rem(me_y + step, ny)
        block = hid.at[at, y]
        return remote(
            block, block, hy_s.at[at, step - 1], hy_r.at[at, step - 1], ra=me_z * ny + to
        )

    spread = int(length * SPREAD) // 16 * 16
    both, own = pl.ds(0, spread), pl.ds(spread, length - spread)

    def hz_copy(at, end):
        rows_of = hid.at[at, :, both]
        return remote(rows_of, rows_of, hz_s.at[at], hz_r.at[at], ra=along(1 - end))

    def own_copy(at, end):
        rows_of = hid.at[at, me_y, own]
        return remote(rows_of, rows_of, nz_s.at[at], nz_r.at[at], ra=along(1 - end))

    def cross_copy(at, step, y):
        rows_of = hid.at[at, y, own]
        return remote(
            rows_of, rows_of, ny_s.at[at, step - 1], ny_r.at[at, step - 1],
            ra=me_z * ny + lax.rem(me_y + step, ny),
        )

    def core_copy(layer, g):
        return remote(
            c_out.at[layer, g], c_in.at[layer, g], c_s.at[layer, g], c_r.at[layer, g],
            cb=me_cb + 1 - 2 * core,
        )

    def sum_copy(layer, g, step, source):
        piece = c_sum.at[layer, g, source]
        return remote(
            piece, piece, cs_s.at[layer, g, step - 1], cs_r.at[layer, g, step - 1],
            cb=lax.rem(chip + step, chips) * CORES + core,
        )

    def all_copy(layer, g, source):
        piece = c_all.at[layer, g, source]
        return remote(
            piece, piece, ca_s.at[layer, g], ca_r.at[layer, g], cb=me_cb + 1 - 2 * core
        )

    row_in_seq = lax.broadcasted_iota(jnp.int32, (length, LANES), 0)

    def of_layer(values, layer):
        picked = values[:1]
        for other in range(1, layers):
            picked = jnp.where(layer == other, values[other:other + 1], picked)
        return picked

    def prepare(layer, g):
        values = carried[g]
        squares = jnp.sum(values * values, axis=1, keepdims=True)
        sq_own[layer, g] = jnp.transpose(jnp.broadcast_to(squares, (rows, LANES)))[:1]
        scaled[g] = (values * of_layer(gain_ref[...], layer)).astype(BF16)
        acc[g] = jnp.zeros(acc.shape[1:], F32)

    def send_squares(layer, g):
        for step in range(1, ny):
            square_copy(layer, g, step).start()

    def add_squares(layer, g):
        total = sq_own[layer, g]
        for step in range(1, ny):
            square_copy(layer, g, step).wait_recv()
            total = total + sq_y[layer, g, step - 1]
        sq_sum[layer, g] = total

    def chain_squares(layer, g, end):
        square_along(layer, g, end).wait_recv()
        return sq_sum[layer, g] + sq_z[layer, g, end]

    def scale(layer, g, end):
        total = chain_squares(layer, g, end)
        total = jnp.transpose(jnp.broadcast_to(total, (LANES, rows)))
        inv[g] = lax.rsqrt(total / (n_ra * gain_ref.shape[1]) + EPS)

    def settle_squares(layer, g):
        for step in range(1, ny):
            square_copy(layer, g, step).wait_send()

        @pl.when(me_z > 0)
        def _():
            square_along(layer, g, 0).wait_send()

        @pl.when(me_z < nz - 1)
        def _():
            square_along(layer, g, 1).wait_send()

    def project(layer, g, i, at, end, hop):
        @pl.when(g == 0)
        def _():
            for copy in weight_copies(layer, i)[:2]:
                copy.wait()

        cols = pl.ds(pl.multiple_of(i * width, width), width)
        for half, w_ref in enumerate((gw_ref, uw_ref)):
            product = jnp.dot(scaled[g], w_ref[layer, :, cols], preferred_element_type=F32)
            for unit in range(ny):
                s, b = unit // blocks, unit % blocks
                part[at, unit, :, half * LANES:(half + 1) * LANES] = product[
                    s * length:(s + 1) * length, b * LANES:(b + 1) * LANES
                ].astype(BF16)

        for step in range(1, ny):
            y_copy(at, step).start()

        @pl.when(hop == 0)
        def _():
            wide_copy(at, end).start()

    def add_y(at, copy, span):
        value = part[at, me_y, span].astype(F32)
        for step in range(1, ny):
            copy(at, step).wait_recv()
            value = value + y_in[at, step - 1, span].astype(F32)
        return value

    def add_z(at, end):
        z_copy(at, end).wait_recv()
        return part[at, me_y, first].astype(F32) + z_in[at, 0, first].astype(F32)

    def add_wide(at, end):
        wide_copy(at, end).wait_recv()
        for unit in range(ny):
            total = part[at, unit, rest].astype(F32) + z_in[at, unit, rest].astype(F32)
            part[at, unit, rest] = total.astype(BF16)

    def activate(layer, g, i, at, end):
        value = jnp.concatenate([add_z(at, end), add_y(at, late_copy, rest)], axis=0)
        cols = pl.ds(pl.multiple_of(i * width + block * LANES, LANES), LANES)
        factor = inv[g, pl.ds(pl.multiple_of(seq * length, length), length), :]
        conv = []
        for half, (taps, bias) in enumerate(((gt_ref, gb_ref), (ut_ref, ub_ref))):
            pre = value[:, half * LANES:(half + 1) * LANES] * factor
            pre = pre.astype(BF16).astype(F32)
            last = jnp.where(row_in_seq >= 1, pltpu.roll(pre, 1, 0), 0.0)
            older = jnp.where(row_in_seq >= 2, pltpu.roll(pre, 2, 0), 0.0)
            tap = [of_layer(taps[k, :, cols], layer) for k in range(3)]
            conv.append(
                of_layer(bias[:, cols], layer) + tap[0] * older + tap[1] * last + tap[2] * pre
            )
        gate, up = conv
        hid[at, me_y] = (gate / (1.0 + jnp.exp(-gate)) * up).astype(BF16)
        for step in range(1, ny):
            hy_copy(at, step, me_y).start()
        own_copy(at, end).start()

    def gather_y(at):
        for step in range(1, ny):
            hy_copy(at, step, lax.rem(me_y - step + ny, ny)).wait_recv()

    def down(layer, g, i, at):
        @pl.when(g == 0)
        def _():
            weight_copies(layer, i)[2].wait()

        depth = pl.ds(pl.multiple_of(i * width, width), width)
        units = [hid[at, unit] for unit in range(ny)]
        hidden = jnp.concatenate(
            [jnp.concatenate(units[s:s + blocks], axis=1) for s in range(0, ny, blocks)], axis=0
        )
        acc[g] += jnp.dot(hidden, dw_ref[layer, depth, :], preferred_element_type=F32)

    def settle(at, end, hop):
        for step in range(1, ny):
            y_copy(at, step).wait_send()

        @pl.when(hop < nz - 1)
        def _():
            z_copy(at, end).wait_send()
            wide_copy(at, end).wait_send()

        @pl.when(hop == nz - 1)
        def _():
            for step in range(1, ny):
                late_copy(at, step).wait_send()
                hy_copy(at, step, me_y).wait_send()

        @pl.when(hop > 0)
        def _():
            hz_copy(at, end).wait_send()
            own_copy(at, end).wait_send()

        @pl.when(hop < nz - 1)
        def _():
            for step in range(1, ny):
                cross_copy(at, step, me_y).wait_send()

    def half_of(which):
        return pl.ds(pl.multiple_of(which * half_rows, half_rows), half_rows)

    def core_sum(layer, g):
        c_out[layer, g] = acc[g, half_of(1 - core), :].astype(BF16)
        core_copy(layer, g).start()

    def chip_sum(layer, g):
        core_copy(layer, g).wait()
        value = acc[g, half_of(core), :] + c_in[layer, g].astype(F32)
        c_sum[layer, g, chip] = value.astype(BF16)
        for step in range(1, chips):
            sum_copy(layer, g, step, chip).start()

    def total_sum(layer, g):
        for step in range(1, chips):
            sum_copy(layer, g, step, lax.rem(chip - step + chips, chips)).wait_recv()
            sum_copy(layer, g, step, chip).wait_send()
        value = c_sum[layer, g, 0].astype(F32)
        for other in range(1, chips):
            value = value + c_sum[layer, g, other].astype(F32)
        c_all[layer, g, core] = value.astype(BF16)
        all_copy(layer, g, core).start()

    def finish(layer, g):
        all_copy(layer, g, 1 - core).wait_recv()
        all_copy(layer, g, core).wait_send()
        settle_squares(layer, g)
        branch = c_all[layer, g].reshape(rows, c_all.shape[4]).astype(F32)
        carried[g] = RESID * carried[g] + branch

        @pl.when(layer < layers - 1)
        def _():
            prepare(layer + 1, g)
            send_squares(layer + 1, g)

        @pl.when(layer == layers - 1)
        def _():
            out_ref[g] = carried[g].astype(out_ref.dtype)

    def enter(g):
        carried[g] = tok_ref[g].astype(F32)
        prepare(0, g)

    for copy in inputs:
        copy.wait()
    enter(0)
    pl.semaphore_wait(barrier, guests)
    send_squares(0, 0)

    act_lag = LAG_Y + LAG_Z * (nz - 1)
    gather_lag = act_lag + LAG_HY
    down_lag = gather_lag + LAG_HZ * (nz - 1)
    total_lag = down_lag + TAIL_END
    stride = max(per_layer, chunks + total_lag)
    stride += stride % 2
    gap = stride - per_layer

    def body(t, _):
        odd = lax.rem(t, 2)
        towards = odd, 1 - odd
        hops = [jnp.where(end == 0, nz - 1 - me_z, me_z) for end in towards]

        def place(lag):
            spot = t - lag
            layer = 0
            for other in range(1, layers):
                layer = layer + jnp.where(spot >= other * stride, 1, 0)
            at = spot - layer * gap
            active = (spot >= 0) & (at < (layer + 1) * per_layer)
            return active, at, towards[lag % 2], hops[lag % 2], layer

        def split_up(at, layer):
            q = at - layer * per_layer
            g = lax.div(q, chunks)
            return g, q - g * chunks

        for lag, stage in ((TAIL_END, finish), (TAIL_SUM, total_sum), (TAIL_CHIP, chip_sum)):
            active, at, end, hop, layer = place(down_lag + lag)

            @pl.when(active)
            def _():
                g, i = split_up(at, layer)

                @pl.when(i == chunks - 1)
                def _():
                    stage(layer, g)

        active, at, end, hop, layer = place(0)

        @pl.when(active)
        def _():
            g, i = split_up(at, layer)

            @pl.when((layer == 0) & (i == 0) & (g > 0))
            def _():
                enter(g)
                send_squares(0, g)

            project(layer, g, i, at, end, hop)

        for far in range(nz - 1, 0, -1):
            active, at, end, hop, layer = place(act_lag + LAG_HZ * far)

            @pl.when(active & (hop == nz - 1 - far))
            def _():
                own_copy(at, end).wait_recv()
                if far < nz - 1:
                    own_copy(at, end).start()
                for step in range(1, ny):
                    cross_copy(at, step, me_y).start()

        for far in range(nz - 2, 0, -1):
            active, at, end, hop, layer = place(gather_lag + LAG_HZ * far)

            @pl.when(active & (hop == nz - 1 - far))
            def _():
                hz_copy(at, end).wait_recv()
                hz_copy(at, end).start()

        active, at, end, hop, layer = place(gather_lag)

        @pl.when(active & (hop == nz - 1))
        def _():
            gather_y(at)
            hz_copy(at, end).start()

        active, at, end, hop, layer = place(act_lag)

        @pl.when(active)
        def _():
            g, i = split_up(at, layer)

            @pl.when((i < 2) & (hop == nz - 1))
            def _():
                scale(layer, g, end)

            @pl.when(hop == nz - 1)
            def _():
                activate(layer, g, i, at, end)

        active, at, end, hop, layer = place(LAG_Z * (nz - 1))

        @pl.when(active & (hop == nz - 1))
        def _():
            add_wide(at, end)
            for step in range(1, ny):
                late_copy(at, step).start()

        for k in range(nz - 2, 0, -1):
            active, at, end, hop, layer = place(LAG_Z * k)

            @pl.when(active & (hop == k))
            def _():
                add_wide(at, end)
                wide_copy(at, end).start()

            active, at, end, hop, layer = place(LAG_Y + LAG_Z * k)

            @pl.when(active & (hop == k))
            def _():
                part[at, me_y, first] = add_z(at, end).astype(BF16)
                z_copy(at, end).start()
                g, i = split_up(at, layer)

                @pl.when(i < 2)
                def _():
                    sq_fwd[layer, g, end] = chain_squares(layer, g, end)
                    square_along(layer, g, end).start()

        active, at, end, hop, layer = place(LAG_Y)

        @pl.when(active)
        def _():
            part[at, me_y, first] = add_y(at, y_copy, first).astype(BF16)

            @pl.when(hop == 0)
            def _():
                z_copy(at, end).start()

            g, i = split_up(at, layer)

            @pl.when(i == 0)
            def _():
                add_squares(layer, g)

            @pl.when((i < 2) & (hop == 0))
            def _():
                sq_fwd[layer, g, end] = sq_sum[layer, g]
                square_along(layer, g, end).start()

        active, at, end, hop, layer = place(down_lag)

        @pl.when(active)
        def _():
            g, i = split_up(at, layer)

            @pl.when(hop == 0)
            def _():
                hz_copy(at, end).wait_recv()

            @pl.when(hop < nz - 1)
            def _():
                for step in range(1, ny):
                    cross_copy(at, step, lax.rem(me_y - step + ny, ny)).wait_recv()

            down(layer, g, i, at)
            settle(at, end, hop)

            @pl.when(i == chunks - 1)
            def _():
                core_sum(layer, g)

        return 0

    lax.fori_loop(0, stride * (layers - 1) + per_layer + total_lag, body, 0)


def per_device(n_ra, n_cb, tokens, gain, gw, uw, gt, ut, gb, ub, dw):
    seqs, length, d = tokens.shape
    layers, _, ff = gw.shape
    nz = seqs
    ny = n_ra // nz
    blocks = ny if ff % (ny * LANES) == 0 else 1
    width = blocks * LANES
    groups = seqs * blocks // ny
    rows = seqs * length // groups
    chunks = ff // width
    n = layers * groups * chunks
    dims = (n_ra, n_cb, nz, groups, rows, length, layers, width, chunks)
    vmem = pl.BlockSpec(memory_space=pltpu.VMEM)
    hbm = pl.BlockSpec(memory_space=pl.ANY)
    dma = pltpu.SemaphoreType.DMA
    ys = max(ny - 1, 1)
    half, chips = rows // CORES, n_cb // CORES
    taps = gt.shape[1]
    scratch = [
        pltpu.VMEM((groups, rows, d), tokens.dtype),
        pltpu.VMEM(gain.shape, F32),
        pltpu.VMEM((taps, layers, ff), F32),
        pltpu.VMEM((taps, layers, ff), F32),
        pltpu.VMEM(gb.shape, F32),
        pltpu.VMEM(ub.shape, F32),
        pltpu.VMEM((layers, d, ff), BF16),
        pltpu.VMEM((layers, d, ff), BF16),
        pltpu.VMEM((layers, ff, d), BF16),
        pltpu.VMEM((groups, rows, d), F32),
        pltpu.VMEM((groups, rows, d), BF16),
        pltpu.VMEM((groups, rows, LANES), F32),
        pltpu.VMEM((groups, rows, d), F32),
        pltpu.VMEM((layers, groups, 1, rows), F32),
        pltpu.VMEM((layers, groups, ys, 1, rows), F32),
        pltpu.VMEM((layers, groups, 1, rows), F32),
        pltpu.VMEM((layers, groups, 2, 1, rows), F32),
        pltpu.VMEM((layers, groups, 2, 1, rows), F32),
        pltpu.VMEM((n, ny, length, 2 * LANES), BF16),
        pltpu.VMEM((n, ys, length, 2 * LANES), BF16),
        pltpu.VMEM((n, ny, length, 2 * LANES), BF16),
        pltpu.VMEM((n, ny, length, LANES), BF16),
        pltpu.VMEM((layers, groups, half, d), BF16),
        pltpu.VMEM((layers, groups, half, d), BF16),
        pltpu.VMEM((layers, groups, chips, half, d), BF16),
        pltpu.VMEM((layers, groups, CORES, half, d), BF16),
        dma((6,)),
        dma((layers, chunks, 3)),
        dma((layers, groups, ys)), dma((layers, groups, ys)),
        dma((layers, groups, 2)), dma((layers, groups, 2)),
        dma((n, ys)), dma((n, ys)),
        dma((n,)), dma((n,)),
        dma((n,)), dma((n,)),
        dma((n, ys)), dma((n, ys)),
        dma((n, ys)), dma((n, ys)),
        dma((n,)), dma((n,)),
        dma((n,)), dma((n,)),
        dma((n, ys)), dma((n, ys)),
        dma((layers, groups)), dma((layers, groups)),
        dma((layers, groups, max(chips - 1, 1))), dma((layers, groups, max(chips - 1, 1))),
        dma((layers, groups)), dma((layers, groups)),
    ]
    out = pl.pallas_call(
        functools.partial(kernel, dims),
        out_shape=jax.ShapeDtypeStruct((groups, rows, d), tokens.dtype),
        in_specs=[hbm] * 9,
        out_specs=vmem,
        scratch_shapes=scratch,
        compiler_params=pltpu.CompilerParams(
            collective_id=0, has_side_effects=True, vmem_limit_bytes=60 * 1024 * 1024
        ),
        name="blocks",
    )(
        tokens.reshape(groups, rows, d), gain, gw, uw,
        jnp.transpose(gt, (1, 0, 2)), jnp.transpose(ut, (1, 0, 2)), gb, ub, dw,
    )
    return out.reshape(tokens.shape)


def solution(mesh):
    in_specs = (
        P(None, None, "ra"),
        P(None, "ra"),
        P(None, "ra", "cb"),
        P(None, "ra", "cb"),
        P(None, None, "cb"),
        P(None, None, "cb"),
        P(None, "cb"),
        P(None, "cb"),
        P(None, "cb", "ra"),
    )
    return jax.shard_map(
        functools.partial(per_device, mesh.shape["ra"], mesh.shape["cb"]),
        mesh=mesh, in_specs=in_specs, out_specs=P(None, None, "ra"), check_vma=False,
    )
```

```python
import functools

import jax
import jax.numpy as jnp
from jax import lax
from jax.experimental import pallas as pl
from jax.experimental.pallas import tpu as pltpu
from jax.sharding import PartitionSpec as P

EPS = 1e-06
RESID = 0.5
LANES = 128
CORES = 2
LAG_Y, LAG_Z, LAG_HY, LAG_HZ = 4, 4, 4, 4
TAIL_CHIP, TAIL_SUM, TAIL_END = 1, 4, 5
SPLIT, SPREAD = 1 / 2, 1 / 2

MESH = pl.DeviceIdType.MESH
F32, BF16 = jnp.float32, jnp.bfloat16


def kernel(
    dims,
    tok_hbm, gain_hbm, gw_hbm, uw_hbm, gt_hbm, ut_hbm, gb_hbm, ub_hbm, dw_hbm,
    out_hbm,
    out_ref, tok_ref, gain_ref, gt_ref, ut_ref, gb_ref, ub_ref,
    gw_ref, uw_ref, dw_ref, carried, scaled, inv, acc,
    sq_own, sq_y, sq_sum, sq_fwd, sq_z, part, y_in, z_in, hid, c_out, c_in, c_sum, c_all,
    o_sem, i_sem, w_sem, sq_s, sq_r, sz_s, sz_r, y_s, y_r, z_s, z_r, wz_s, wz_r, wy_s, wy_r, hy_s, hy_r, hz_s, hz_r, nz_s, nz_r, ny_s, ny_r, c_s, c_r, cs_s, cs_r, ca_s, ca_r,
):
    n_ra, n_cb, nz, groups, rows, length, layers, width, chunks = dims
    ny = n_ra // nz
    blocks = width // LANES
    per_layer = groups * chunks
    half_rows = rows // CORES
    me_ra = lax.axis_index("ra")
    me_cb = lax.axis_index("cb")
    me_z, me_y = me_ra // ny, me_ra % ny
    core, chip, chips = me_cb % CORES, me_cb // CORES, n_cb // CORES
    seq, block = me_y // blocks, me_y % blocks

    def weight_copies(layer, i):
        cols = pl.ds(pl.multiple_of(i * width, width), width)
        return [
            pltpu.make_async_copy(
                gw_hbm.at[layer, :, cols], gw_ref.at[layer, :, cols], w_sem.at[layer, i, 0]
            ),
            pltpu.make_async_copy(
                uw_hbm.at[layer, :, cols], uw_ref.at[layer, :, cols], w_sem.at[layer, i, 1]
            ),
            pltpu.make_async_copy(
                dw_hbm.at[layer, cols], dw_ref.at[layer, cols], w_sem.at[layer, i, 2]
            ),
        ]

    barrier = pltpu.get_barrier_semaphore()
    def greet(**where):
        pl.semaphore_signal(barrier, inc=1, device_id=where, device_id_type=MESH)

    for step in range(1, ny):
        greet(ra=me_z * ny + lax.rem(me_y + step, ny))
    for step in range(1, chips):
        greet(cb=lax.rem(chip + step, chips) * CORES + core)
    greet(cb=me_cb + 1 - 2 * core)

    @pl.when(me_z > 0)
    def _():
        greet(ra=me_ra - ny)

    @pl.when(me_z < nz - 1)
    def _():
        greet(ra=me_ra + ny)

    guests = ny + chips - 1 + jnp.where(me_z > 0, 1, 0) + jnp.where(me_z < nz - 1, 1, 0)

    inputs = [
        pltpu.make_async_copy(source, target, i_sem.at[k])
        for k, (source, target) in enumerate((
            (tok_hbm, tok_ref), (gain_hbm, gain_ref), (gt_hbm, gt_ref), (ut_hbm, ut_ref),
            (gb_hbm, gb_ref), (ub_hbm, ub_ref),
        ))
    ]
    for copy in inputs:
        copy.start()

    for layer in range(layers):
        def fetch(i, _, layer=layer):
            for copy in weight_copies(layer, i):
                copy.start()
            return 0

        lax.fori_loop(0, chunks, fetch, 0)

    def remote(src, dst, send, recv, **where):
        return pltpu.make_async_remote_copy(
            src_ref=src, dst_ref=dst, send_sem=send, recv_sem=recv,
            device_id=where, device_id_type=MESH,
        )

    def square_copy(layer, g, step):
        return remote(
            sq_own.at[layer, g], sq_y.at[layer, g, step - 1],
            sq_s.at[layer, g, step - 1], sq_r.at[layer, g, step - 1],
            ra=me_z * ny + lax.rem(me_y + step, ny),
        )

    def square_along(layer, g, end):
        return remote(
            sq_fwd.at[layer, g, end], sq_z.at[layer, g, end],
            sz_s.at[layer, g, end], sz_r.at[layer, g, end], ra=along(end),
        )

    split = int(length * SPLIT) // 16 * 16
    first, rest = pl.ds(0, split), pl.ds(split, length - split)

    def y_copy(at, step):
        to = lax.rem(me_y + step, ny)
        return remote(
            part.at[at, to, first], y_in.at[at, step - 1, first],
            y_s.at[step - 1], y_r.at[at, step - 1], ra=me_z * ny + to,
        )

    def late_copy(at, step):
        to = lax.rem(me_y + step, ny)
        return remote(
            part.at[at, to, rest], y_in.at[at, step - 1, rest],
            wy_s.at[step - 1], wy_r.at[at, step - 1], ra=me_z * ny + to,
        )

    def along(end):
        return lax.rem(me_z + 2 * end - 1 + nz, nz) * ny + me_y

    def z_copy(at, end):
        return remote(
            part.at[at, me_y, first], z_in.at[at, 0, first], z_s.at[end], z_r.at[at],
            ra=along(end),
        )

    def wide_copy(at, end):
        return remote(
            part.at[at, :, rest], z_in.at[at, :, rest], wz_s.at[end], wz_r.at[at], ra=along(end)
        )

    def hy_copy(at, step, y):
        to = lax.rem(me_y + step, ny)
        block = hid.at[at, y]
        return remote(
            block, block, hy_s.at[step - 1], hy_r.at[at, step - 1], ra=me_z * ny + to
        )

    spread = int(length * SPREAD) // 16 * 16
    both, own = pl.ds(0, spread), pl.ds(spread, length - spread)

    def hz_copy(at, end):
        rows_of = hid.at[at, :, both]
        return remote(rows_of, rows_of, hz_s.at[end], hz_r.at[at], ra=along(1 - end))

    def own_copy(at, end):
        rows_of = hid.at[at, me_y, own]
        return remote(rows_of, rows_of, nz_s.at[end], nz_r.at[at], ra=along(1 - end))

    def cross_copy(at, end, step, y):
        rows_of = hid.at[at, y, own]
        return remote(
            rows_of, rows_of, ny_s.at[end, step - 1], ny_r.at[at, step - 1],
            ra=me_z * ny + lax.rem(me_y + step, ny),
        )

    def core_copy(layer, g):
        return remote(
            c_out.at[layer, g], c_in.at[layer, g], c_s.at[layer, g], c_r.at[layer, g],
            cb=me_cb + 1 - 2 * core,
        )

    def sum_copy(layer, g, step, source):
        piece = c_sum.at[layer, g, source]
        return remote(
            piece, piece, cs_s.at[layer, g, step - 1], cs_r.at[layer, g, step - 1],
            cb=lax.rem(chip + step, chips) * CORES + core,
        )

    def all_copy(layer, g, source):
        piece = c_all.at[layer, g, source]
        return remote(
            piece, piece, ca_s.at[layer, g], ca_r.at[layer, g], cb=me_cb + 1 - 2 * core
        )

    row_in_seq = lax.broadcasted_iota(jnp.int32, (length, LANES), 0)

    def of_layer(values, layer):
        picked = values[:1]
        for other in range(1, layers):
            picked = jnp.where(layer == other, values[other:other + 1], picked)
        return picked

    def prepare(layer, g):
        values = carried[g]
        squares = jnp.sum(values * values, axis=1, keepdims=True)
        sq_own[layer, g] = jnp.transpose(jnp.broadcast_to(squares, (rows, LANES)))[:1]
        scaled[g] = (values * of_layer(gain_ref[...], layer)).astype(BF16)
        acc[g] = jnp.zeros(acc.shape[1:], F32)

    def send_squares(layer, g):
        for step in range(1, ny):
            square_copy(layer, g, step).start()

    def add_squares(layer, g):
        total = sq_own[layer, g]
        for step in range(1, ny):
            square_copy(layer, g, step).wait_recv()
            total = total + sq_y[layer, g, step - 1]
        sq_sum[layer, g] = total

    def chain_squares(layer, g, end):
        square_along(layer, g, end).wait_recv()
        return sq_sum[layer, g] + sq_z[layer, g, end]

    def scale(layer, g, end):
        total = chain_squares(layer, g, end)
        total = jnp.transpose(jnp.broadcast_to(total, (LANES, rows)))
        inv[g] = lax.rsqrt(total / (n_ra * gain_ref.shape[1]) + EPS)

    def settle_squares(layer, g):
        for step in range(1, ny):
            square_copy(layer, g, step).wait_send()

        @pl.when(me_z > 0)
        def _():
            square_along(layer, g, 0).wait_send()

        @pl.when(me_z < nz - 1)
        def _():
            square_along(layer, g, 1).wait_send()

    def project(layer, g, i, at, end, hop):
        @pl.when(g == 0)
        def _():
            for copy in weight_copies(layer, i)[:2]:
                copy.wait()

        cols = pl.ds(pl.multiple_of(i * width, width), width)
        for half, w_ref in enumerate((gw_ref, uw_ref)):
            product = jnp.dot(scaled[g], w_ref[layer, :, cols], preferred_element_type=F32)
            for unit in range(ny):
                s, b = unit // blocks, unit % blocks
                part[at, unit, :, half * LANES:(half + 1) * LANES] = product[
                    s * length:(s + 1) * length, b * LANES:(b + 1) * LANES
                ].astype(BF16)

        for step in range(1, ny):
            y_copy(at, step).start()

        @pl.when(hop == 0)
        def _():
            wide_copy(at, end).start()

    def add_y(at, copy, span):
        value = part[at, me_y, span].astype(F32)
        for step in range(1, ny):
            copy(at, step).wait_recv()
            value = value + y_in[at, step - 1, span].astype(F32)
        return value

    def add_z(at, end):
        z_copy(at, end).wait_recv()
        return part[at, me_y, first].astype(F32) + z_in[at, 0, first].astype(F32)

    def add_wide(at, end):
        wide_copy(at, end).wait_recv()
        for unit in range(ny):
            total = part[at, unit, rest].astype(F32) + z_in[at, unit, rest].astype(F32)
            part[at, unit, rest] = total.astype(BF16)

    def activate(layer, g, i, at, end):
        value = jnp.concatenate([add_z(at, end), add_y(at, late_copy, rest)], axis=0)
        cols = pl.ds(pl.multiple_of(i * width + block * LANES, LANES), LANES)
        factor = inv[g, pl.ds(pl.multiple_of(seq * length, length), length), :]
        conv = []
        for half, (taps, bias) in enumerate(((gt_ref, gb_ref), (ut_ref, ub_ref))):
            pre = value[:, half * LANES:(half + 1) * LANES] * factor
            pre = pre.astype(BF16).astype(F32)
            last = jnp.where(row_in_seq >= 1, pltpu.roll(pre, 1, 0), 0.0)
            older = jnp.where(row_in_seq >= 2, pltpu.roll(pre, 2, 0), 0.0)
            tap = [of_layer(taps[k, :, cols], layer) for k in range(3)]
            conv.append(
                of_layer(bias[:, cols], layer) + tap[0] * older + tap[1] * last + tap[2] * pre
            )
        gate, up = conv
        hid[at, me_y] = (gate / (1.0 + jnp.exp(-gate)) * up).astype(BF16)
        for step in range(1, ny):
            hy_copy(at, step, me_y).start()
        own_copy(at, end).start()

    def gather_y(at):
        for step in range(1, ny):
            hy_copy(at, step, lax.rem(me_y - step + ny, ny)).wait_recv()

    def down(layer, g, i, at):
        @pl.when(g == 0)
        def _():
            weight_copies(layer, i)[2].wait()

        depth = pl.ds(pl.multiple_of(i * width, width), width)
        units = [hid[at, unit] for unit in range(ny)]
        hidden = jnp.concatenate(
            [jnp.concatenate(units[s:s + blocks], axis=1) for s in range(0, ny, blocks)], axis=0
        )
        acc[g] += jnp.dot(hidden, dw_ref[layer, depth, :], preferred_element_type=F32)

    def sent(ref, semaphore):
        remote(ref, ref, semaphore, semaphore, cb=me_cb + 1 - 2 * core).wait_send()

    def settle():
        for step in range(1, ny):
            sent(y_in.at[:, step - 1, first], y_s.at[step - 1])
        for end in range(2):
            many = pl.ds(0, layers * ((per_layer + 1 - end) // 2))

            @pl.when(me_z == end * (nz - 1))
            def _():
                for step in range(1, ny):
                    sent(y_in.at[many, step - 1, rest], wy_s.at[step - 1])
                    sent(hid.at[many, 0], hy_s.at[step - 1])

            @pl.when(me_z != end * (nz - 1))
            def _():
                sent(z_in.at[many, 0, first], z_s.at[end])
                sent(z_in.at[many, :, rest], wz_s.at[end])
                for step in range(1, ny):
                    sent(hid.at[many, 0, own], ny_s.at[end, step - 1])

            @pl.when(me_z != (1 - end) * (nz - 1))
            def _():
                sent(hid.at[many, :, both], hz_s.at[end])
                sent(hid.at[many, 0, own], nz_s.at[end])

    def half_of(which):
        return pl.ds(pl.multiple_of(which * half_rows, half_rows), half_rows)

    def core_sum(layer, g):
        c_out[layer, g] = acc[g, half_of(1 - core), :].astype(BF16)
        core_copy(layer, g).start()

    def chip_sum(layer, g):
        core_copy(layer, g).wait()
        value = acc[g, half_of(core), :] + c_in[layer, g].astype(F32)
        c_sum[layer, g, chip] = value.astype(BF16)
        for step in range(1, chips):
            sum_copy(layer, g, step, chip).start()

    def total_sum(layer, g):
        for step in range(1, chips):
            sum_copy(layer, g, step, lax.rem(chip - step + chips, chips)).wait_recv()
            sum_copy(layer, g, step, chip).wait_send()
        value = c_sum[layer, g, 0].astype(F32)
        for other in range(1, chips):
            value = value + c_sum[layer, g, other].astype(F32)
        c_all[layer, g, core] = value.astype(BF16)
        all_copy(layer, g, core).start()

    def out_copy(g):
        return pltpu.make_async_copy(out_ref.at[g], out_hbm.at[g], o_sem.at[g])

    def finish(layer, g):
        all_copy(layer, g, 1 - core).wait_recv()
        all_copy(layer, g, core).wait_send()
        settle_squares(layer, g)
        branch = c_all[layer, g].reshape(rows, c_all.shape[4]).astype(F32)
        carried[g] = RESID * carried[g] + branch

        @pl.when(layer < layers - 1)
        def _():
            prepare(layer + 1, g)
            send_squares(layer + 1, g)

        @pl.when(layer == layers - 1)
        def _():
            out_ref[g] = carried[g].astype(out_ref.dtype)
            out_copy(g).start()

    def enter(g):
        carried[g] = tok_ref[g].astype(F32)
        prepare(0, g)

    for copy in inputs:
        copy.wait()
    enter(0)
    pl.semaphore_wait(barrier, guests)
    send_squares(0, 0)

    act_lag = LAG_Y + LAG_Z * (nz - 1)
    gather_lag = act_lag + LAG_HY
    down_lag = gather_lag + LAG_HZ * (nz - 1)
    total_lag = down_lag + TAIL_END
    stride = max(per_layer, chunks + total_lag)
    stride += stride % 2
    gap = stride - per_layer

    def body(t, _):
        odd = lax.rem(t, 2)
        towards = odd, 1 - odd
        hops = [jnp.where(end == 0, nz - 1 - me_z, me_z) for end in towards]

        def place(lag):
            spot = t - lag
            layer = 0
            for other in range(1, layers):
                layer = layer + jnp.where(spot >= other * stride, 1, 0)
            at = spot - layer * gap
            active = (spot >= 0) & (at < (layer + 1) * per_layer)
            return active, at, towards[lag % 2], hops[lag % 2], layer

        def split_up(at, layer):
            q = at - layer * per_layer
            g = lax.div(q, chunks)
            return g, q - g * chunks

        for lag, stage in ((TAIL_END, finish), (TAIL_SUM, total_sum), (TAIL_CHIP, chip_sum)):
            active, at, end, hop, layer = place(down_lag + lag)

            @pl.when(active)
            def _():
                g, i = split_up(at, layer)

                @pl.when(i == chunks - 1)
                def _():
                    stage(layer, g)

        active, at, end, hop, layer = place(0)

        @pl.when(active)
        def _():
            g, i = split_up(at, layer)

            @pl.when((layer == 0) & (i == 0) & (g > 0))
            def _():
                enter(g)
                send_squares(0, g)

            project(layer, g, i, at, end, hop)

        for far in range(nz - 1, 0, -1):
            active, at, end, hop, layer = place(act_lag + LAG_HZ * far)

            @pl.when(active & (hop == nz - 1 - far))
            def _():
                own_copy(at, end).wait_recv()
                if far < nz - 1:
                    own_copy(at, end).start()
                for step in range(1, ny):
                    cross_copy(at, end, step, me_y).start()

        for far in range(nz - 2, 0, -1):
            active, at, end, hop, layer = place(gather_lag + LAG_HZ * far)

            @pl.when(active & (hop == nz - 1 - far))
            def _():
                hz_copy(at, end).wait_recv()
                hz_copy(at, end).start()

        active, at, end, hop, layer = place(gather_lag)

        @pl.when(active & (hop == nz - 1))
        def _():
            gather_y(at)
            hz_copy(at, end).start()

        active, at, end, hop, layer = place(act_lag)

        @pl.when(active)
        def _():
            g, i = split_up(at, layer)

            @pl.when((i < 2) & (hop == nz - 1))
            def _():
                scale(layer, g, end)

            @pl.when(hop == nz - 1)
            def _():
                activate(layer, g, i, at, end)

        active, at, end, hop, layer = place(LAG_Z * (nz - 1))

        @pl.when(active & (hop == nz - 1))
        def _():
            add_wide(at, end)
            for step in range(1, ny):
                late_copy(at, step).start()

        for k in range(nz - 2, 0, -1):
            active, at, end, hop, layer = place(LAG_Z * k)

            @pl.when(active & (hop == k))
            def _():
                add_wide(at, end)
                wide_copy(at, end).start()

            active, at, end, hop, layer = place(LAG_Y + LAG_Z * k)

            @pl.when(active & (hop == k))
            def _():
                part[at, me_y, first] = add_z(at, end).astype(BF16)
                z_copy(at, end).start()
                g, i = split_up(at, layer)

                @pl.when(i < 2)
                def _():
                    sq_fwd[layer, g, end] = chain_squares(layer, g, end)
                    square_along(layer, g, end).start()

        active, at, end, hop, layer = place(LAG_Y)

        @pl.when(active)
        def _():
            part[at, me_y, first] = add_y(at, y_copy, first).astype(BF16)

            @pl.when(hop == 0)
            def _():
                z_copy(at, end).start()

            g, i = split_up(at, layer)

            @pl.when(i == 0)
            def _():
                add_squares(layer, g)

            @pl.when((i < 2) & (hop == 0))
            def _():
                sq_fwd[layer, g, end] = sq_sum[layer, g]
                square_along(layer, g, end).start()

        active, at, end, hop, layer = place(down_lag)

        @pl.when(active)
        def _():
            g, i = split_up(at, layer)

            @pl.when(hop == 0)
            def _():
                hz_copy(at, end).wait_recv()

            @pl.when(hop < nz - 1)
            def _():
                for step in range(1, ny):
                    cross_copy(at, end, step, lax.rem(me_y - step + ny, ny)).wait_recv()

            down(layer, g, i, at)

            @pl.when(i == chunks - 1)
            def _():
                core_sum(layer, g)

        return 0

    lax.fori_loop(0, stride * (layers - 1) + per_layer + total_lag, body, 0)
    settle()
    for g in range(groups):
        out_copy(g).wait()


def per_device(n_ra, n_cb, tokens, gain, gw, uw, gt, ut, gb, ub, dw):
    seqs, length, d = tokens.shape
    layers, _, ff = gw.shape
    nz = seqs
    ny = n_ra // nz
    blocks = ny if ff % (ny * LANES) == 0 else 1
    width = blocks * LANES
    groups = seqs * blocks // ny
    rows = seqs * length // groups
    chunks = ff // width
    n = layers * groups * chunks
    dims = (n_ra, n_cb, nz, groups, rows, length, layers, width, chunks)
    hbm = pl.BlockSpec(memory_space=pl.ANY)
    dma = pltpu.SemaphoreType.DMA
    ys = max(ny - 1, 1)
    half, chips = rows // CORES, n_cb // CORES
    taps = gt.shape[1]
    scratch = [
        pltpu.VMEM((groups, rows, d), tokens.dtype),
        pltpu.VMEM((groups, rows, d), tokens.dtype),
        pltpu.VMEM(gain.shape, F32),
        pltpu.VMEM((taps, layers, ff), F32),
        pltpu.VMEM((taps, layers, ff), F32),
        pltpu.VMEM(gb.shape, F32),
        pltpu.VMEM(ub.shape, F32),
        pltpu.VMEM((layers, d, ff), BF16),
        pltpu.VMEM((layers, d, ff), BF16),
        pltpu.VMEM((layers, ff, d), BF16),
        pltpu.VMEM((groups, rows, d), F32),
        pltpu.VMEM((groups, rows, d), BF16),
        pltpu.VMEM((groups, rows, LANES), F32),
        pltpu.VMEM((groups, rows, d), F32),
        pltpu.VMEM((layers, groups, 1, rows), F32),
        pltpu.VMEM((layers, groups, ys, 1, rows), F32),
        pltpu.VMEM((layers, groups, 1, rows), F32),
        pltpu.VMEM((layers, groups, 2, 1, rows), F32),
        pltpu.VMEM((layers, groups, 2, 1, rows), F32),
        pltpu.VMEM((n, ny, length, 2 * LANES), BF16),
        pltpu.VMEM((n, ys, length, 2 * LANES), BF16),
        pltpu.VMEM((n, ny, length, 2 * LANES), BF16),
        pltpu.VMEM((n, ny, length, LANES), BF16),
        pltpu.VMEM((layers, groups, half, d), BF16),
        pltpu.VMEM((layers, groups, half, d), BF16),
        pltpu.VMEM((layers, groups, chips, half, d), BF16),
        pltpu.VMEM((layers, groups, CORES, half, d), BF16),
        dma((groups,)), dma((6,)),
        dma((layers, chunks, 3)),
        dma((layers, groups, ys)), dma((layers, groups, ys)),
        dma((layers, groups, 2)), dma((layers, groups, 2)),
        dma((ys,)), dma((n, ys)),
        dma((2,)), dma((n,)),
        dma((2,)), dma((n,)),
        dma((ys,)), dma((n, ys)),
        dma((ys,)), dma((n, ys)),
        dma((2,)), dma((n,)),
        dma((2,)), dma((n,)),
        dma((2, ys)), dma((n, ys)),
        dma((layers, groups)), dma((layers, groups)),
        dma((layers, groups, max(chips - 1, 1))), dma((layers, groups, max(chips - 1, 1))),
        dma((layers, groups)), dma((layers, groups)),
    ]
    out = pl.pallas_call(
        functools.partial(kernel, dims),
        out_shape=jax.ShapeDtypeStruct((groups, rows, d), tokens.dtype),
        in_specs=[hbm] * 9,
        out_specs=hbm,
        scratch_shapes=scratch,
        compiler_params=pltpu.CompilerParams(
            collective_id=0, has_side_effects=True, vmem_limit_bytes=60 * 1024 * 1024
        ),
        name="blocks",
    )(
        tokens.reshape(groups, rows, d), gain, gw, uw,
        jnp.transpose(gt, (1, 0, 2)), jnp.transpose(ut, (1, 0, 2)), gb, ub, dw,
    )
    return out.reshape(tokens.shape)


def solution(mesh):
    in_specs = (
        P(None, None, "ra"),
        P(None, "ra"),
        P(None, "ra", "cb"),
        P(None, "ra", "cb"),
        P(None, None, "cb"),
        P(None, None, "cb"),
        P(None, "cb"),
        P(None, "cb"),
        P(None, "cb", "ra"),
    )
    return jax.shard_map(
        functools.partial(per_device, mesh.shape["ra"], mesh.shape["cb"]),
        mesh=mesh, in_specs=in_specs, out_specs=P(None, None, "ra"), check_vma=False,
    )
```

```python
import functools

import jax
import jax.numpy as jnp
from jax import lax
from jax.experimental import pallas as pl
from jax.experimental.pallas import tpu as pltpu
from jax.sharding import PartitionSpec as P

EPS = 1e-06
RESID = 0.5
LANES = 128
CORES = 2
LAG_Y, LAG_Z, LAG_HY, LAG_HZ = 4, 4, 4, 4
TAIL_CHIP, TAIL_SUM, TAIL_END = 1, 4, 5
SPLIT, SPREAD = 5 / 8, 5 / 8

MESH = pl.DeviceIdType.MESH
F32, BF16 = jnp.float32, jnp.bfloat16


def kernel(
    dims,
    tok_hbm, gain_hbm, gw_hbm, uw_hbm, gt_hbm, ut_hbm, gb_hbm, ub_hbm, dw_hbm,
    out_hbm,
    out_ref, tok_ref, gain_ref, gt_ref, ut_ref, gb_ref, ub_ref,
    gw_ref, uw_ref, dw_ref, carried, scaled, inv, acc,
    sq_own, sq_y, sq_sum, sq_fwd, sq_z, part, y_in, z_in, hid, c_out, c_in, c_sum, c_all,
    o_sem, i_sem, w_sem, sq_s, sq_r, sz_s, sz_r, y_s, y_r, z_s, z_r, wz_s, wz_r, wy_s, wy_r, hy_s, hy_r, hz_s, hz_r, nz_s, nz_r, ny_s, ny_r, c_s, c_r, cs_s, cs_r, ca_s, ca_r,
):
    n_ra, n_cb, nz, groups, rows, length, layers, width, chunks = dims
    ny = n_ra // nz
    blocks = width // LANES
    per_layer = groups * chunks
    half_rows = rows // CORES
    me_ra = lax.axis_index("ra")
    me_cb = lax.axis_index("cb")
    me_z, me_y = me_ra // ny, me_ra % ny
    core, chip, chips = me_cb % CORES, me_cb // CORES, n_cb // CORES
    seq, block = me_y // blocks, me_y % blocks

    def weight_copies(layer, i):
        cols = pl.ds(pl.multiple_of(i * width, width), width)
        return [
            pltpu.make_async_copy(
                gw_hbm.at[layer, :, cols], gw_ref.at[layer, :, cols], w_sem.at[layer, i, 0]
            ),
            pltpu.make_async_copy(
                uw_hbm.at[layer, :, cols], uw_ref.at[layer, :, cols], w_sem.at[layer, i, 1]
            ),
            pltpu.make_async_copy(
                dw_hbm.at[layer, cols], dw_ref.at[layer, cols], w_sem.at[layer, i, 2]
            ),
        ]

    barrier = pltpu.get_barrier_semaphore()
    def greet(**where):
        pl.semaphore_signal(barrier, inc=1, device_id=where, device_id_type=MESH)

    for step in range(1, ny):
        greet(ra=me_z * ny + lax.rem(me_y + step, ny))
    for step in range(1, chips):
        greet(cb=lax.rem(chip + step, chips) * CORES + core)
    greet(cb=me_cb + 1 - 2 * core)

    @pl.when(me_z > 0)
    def _():
        greet(ra=me_ra - ny)

    @pl.when(me_z < nz - 1)
    def _():
        greet(ra=me_ra + ny)

    guests = ny + chips - 1 + jnp.where(me_z > 0, 1, 0) + jnp.where(me_z < nz - 1, 1, 0)

    inputs = [
        pltpu.make_async_copy(source, target, i_sem.at[k])
        for k, (source, target) in enumerate((
            (tok_hbm, tok_ref), (gain_hbm, gain_ref), (gt_hbm, gt_ref), (ut_hbm, ut_ref),
            (gb_hbm, gb_ref), (ub_hbm, ub_ref),
        ))
    ]
    for copy in inputs:
        copy.start()

    for layer in range(layers):
        def fetch(i, _, layer=layer):
            for copy in weight_copies(layer, i):
                copy.start()
            return 0

        lax.fori_loop(0, chunks, fetch, 0)

    def remote(src, dst, send, recv, **where):
        return pltpu.make_async_remote_copy(
            src_ref=src, dst_ref=dst, send_sem=send, recv_sem=recv,
            device_id=where, device_id_type=MESH,
        )

    def square_copy(layer, g, step):
        return remote(
            sq_own.at[layer, g], sq_y.at[layer, g, step - 1],
            sq_s.at[layer, g, step - 1], sq_r.at[layer, g, step - 1],
            ra=me_z * ny + lax.rem(me_y + step, ny),
        )

    def square_along(layer, g, end):
        return remote(
            sq_fwd.at[layer, g, end], sq_z.at[layer, g, end],
            sz_s.at[layer, g, end], sz_r.at[layer, g, end], ra=along(end),
        )

    split = int(length * SPLIT) // 16 * 16
    first, rest = pl.ds(0, split), pl.ds(split, length - split)

    def y_copy(at, step):
        to = lax.rem(me_y + step, ny)
        return remote(
            part.at[at, to, first], y_in.at[at, step - 1, first],
            y_s.at[step - 1], y_r.at[at, step - 1], ra=me_z * ny + to,
        )

    def late_copy(at, step):
        to = lax.rem(me_y + step, ny)
        return remote(
            part.at[at, to, rest], y_in.at[at, step - 1, rest],
            wy_s.at[step - 1], wy_r.at[at, step - 1], ra=me_z * ny + to,
        )

    def along(end):
        return lax.rem(me_z + 2 * end - 1 + nz, nz) * ny + me_y

    def z_copy(at, end):
        return remote(
            part.at[at, me_y, first], z_in.at[at, 0, first], z_s.at[end], z_r.at[at],
            ra=along(end),
        )

    def wide_copy(at, end):
        return remote(
            part.at[at, :, rest], z_in.at[at, :, rest], wz_s.at[end], wz_r.at[at], ra=along(end)
        )

    def hy_copy(at, step, y):
        to = lax.rem(me_y + step, ny)
        block = hid.at[at, y]
        return remote(
            block, block, hy_s.at[step - 1], hy_r.at[at, step - 1], ra=me_z * ny + to
        )

    spread = int(length * SPREAD) // 16 * 16
    both, own = pl.ds(0, spread), pl.ds(spread, length - spread)

    def hz_copy(at, end):
        rows_of = hid.at[at, :, both]
        return remote(rows_of, rows_of, hz_s.at[end], hz_r.at[at], ra=along(1 - end))

    def own_copy(at, end):
        rows_of = hid.at[at, me_y, own]
        return remote(rows_of, rows_of, nz_s.at[end], nz_r.at[at], ra=along(1 - end))

    def cross_copy(at, end, step, y):
        rows_of = hid.at[at, y, own]
        return remote(
            rows_of, rows_of, ny_s.at[end, step - 1], ny_r.at[at, step - 1],
            ra=me_z * ny + lax.rem(me_y + step, ny),
        )

    def core_copy(layer, g):
        return remote(
            c_out.at[layer, g], c_in.at[layer, g], c_s.at[layer, g], c_r.at[layer, g],
            cb=me_cb + 1 - 2 * core,
        )

    def sum_copy(layer, g, step, source):
        piece = c_sum.at[layer, g, source]
        return remote(
            piece, piece, cs_s.at[layer, g, step - 1], cs_r.at[layer, g, step - 1],
            cb=lax.rem(chip + step, chips) * CORES + core,
        )

    def all_copy(layer, g, source):
        piece = c_all.at[layer, g, source]
        return remote(
            piece, piece, ca_s.at[layer, g], ca_r.at[layer, g], cb=me_cb + 1 - 2 * core
        )

    row_in_seq = lax.broadcasted_iota(jnp.int32, (length, LANES), 0)

    def of_layer(values, layer):
        picked = values[:1]
        for other in range(1, layers):
            picked = jnp.where(layer == other, values[other:other + 1], picked)
        return picked

    def prepare(layer, g):
        values = carried[g]
        squares = jnp.sum(values * values, axis=1, keepdims=True)
        sq_own[layer, g] = jnp.transpose(jnp.broadcast_to(squares, (rows, LANES)))[:1]
        scaled[g] = (values * of_layer(gain_ref[...], layer)).astype(BF16)
        acc[g] = jnp.zeros(acc.shape[1:], F32)

    def send_squares(layer, g):
        for step in range(1, ny):
            square_copy(layer, g, step).start()

    def add_squares(layer, g):
        total = sq_own[layer, g]
        for step in range(1, ny):
            square_copy(layer, g, step).wait_recv()
            total = total + sq_y[layer, g, step - 1]
        sq_sum[layer, g] = total

    def chain_squares(layer, g, end):
        square_along(layer, g, end).wait_recv()
        return sq_sum[layer, g] + sq_z[layer, g, end]

    def scale(layer, g, end):
        total = chain_squares(layer, g, end)
        total = jnp.transpose(jnp.broadcast_to(total, (LANES, rows)))
        inv[g] = lax.rsqrt(total / (n_ra * gain_ref.shape[1]) + EPS)

    def settle_squares(layer, g):
        for step in range(1, ny):
            square_copy(layer, g, step).wait_send()

        @pl.when(me_z > 0)
        def _():
            square_along(layer, g, 0).wait_send()

        @pl.when(me_z < nz - 1)
        def _():
            square_along(layer, g, 1).wait_send()

    def project(layer, g, i, at, end, hop):
        @pl.when(g == 0)
        def _():
            for copy in weight_copies(layer, i)[:2]:
                copy.wait()

        cols = pl.ds(pl.multiple_of(i * width, width), width)
        for half, w_ref in enumerate((gw_ref, uw_ref)):
            product = jnp.dot(scaled[g], w_ref[layer, :, cols], preferred_element_type=F32)
            for unit in range(ny):
                s, b = unit // blocks, unit % blocks
                part[at, unit, :, half * LANES:(half + 1) * LANES] = product[
                    s * length:(s + 1) * length, b * LANES:(b + 1) * LANES
                ].astype(BF16)

        for step in range(1, ny):
            y_copy(at, step).start()

        @pl.when(hop == 0)
        def _():
            wide_copy(at, end).start()

    def add_y(at, copy, span):
        value = part[at, me_y, span].astype(F32)
        for step in range(1, ny):
            copy(at, step).wait_recv()
            value = value + y_in[at, step - 1, span].astype(F32)
        return value

    def add_z(at, end):
        z_copy(at, end).wait_recv()
        return part[at, me_y, first].astype(F32) + z_in[at, 0, first].astype(F32)

    def add_wide(at, end):
        wide_copy(at, end).wait_recv()
        for unit in range(ny):
            total = part[at, unit, rest].astype(F32) + z_in[at, unit, rest].astype(F32)
            part[at, unit, rest] = total.astype(BF16)

    def activate(layer, g, i, at, end):
        value = jnp.concatenate([add_z(at, end), add_y(at, late_copy, rest)], axis=0)
        cols = pl.ds(pl.multiple_of(i * width + block * LANES, LANES), LANES)
        factor = inv[g, pl.ds(pl.multiple_of(seq * length, length), length), :]
        conv = []
        for half, (taps, bias) in enumerate(((gt_ref, gb_ref), (ut_ref, ub_ref))):
            pre = value[:, half * LANES:(half + 1) * LANES] * factor
            pre = pre.astype(BF16).astype(F32)
            last = jnp.where(row_in_seq >= 1, pltpu.roll(pre, 1, 0), 0.0)
            older = jnp.where(row_in_seq >= 2, pltpu.roll(pre, 2, 0), 0.0)
            tap = [of_layer(taps[k, :, cols], layer) for k in range(3)]
            conv.append(
                of_layer(bias[:, cols], layer) + tap[0] * older + tap[1] * last + tap[2] * pre
            )
        gate, up = conv
        hid[at, me_y] = (gate / (1.0 + jnp.exp(-gate)) * up).astype(BF16)
        for step in range(1, ny):
            hy_copy(at, step, me_y).start()
        own_copy(at, end).start()

    def gather_y(at):
        for step in range(1, ny):
            hy_copy(at, step, lax.rem(me_y - step + ny, ny)).wait_recv()

    def down(layer, g, i, at):
        @pl.when(g == 0)
        def _():
            weight_copies(layer, i)[2].wait()

        depth = pl.ds(pl.multiple_of(i * width, width), width)
        units = [hid[at, unit] for unit in range(ny)]
        hidden = jnp.concatenate(
            [jnp.concatenate(units[s:s + blocks], axis=1) for s in range(0, ny, blocks)], axis=0
        )
        acc[g] += jnp.dot(hidden, dw_ref[layer, depth, :], preferred_element_type=F32)

    def sent(ref, semaphore):
        remote(ref, ref, semaphore, semaphore, cb=me_cb + 1 - 2 * core).wait_send()

    def settle():
        for step in range(1, ny):
            sent(y_in.at[:, step - 1, first], y_s.at[step - 1])
        for end in range(2):
            many = pl.ds(0, layers * ((per_layer + 1 - end) // 2))

            @pl.when(me_z == end * (nz - 1))
            def _():
                for step in range(1, ny):
                    sent(y_in.at[many, step - 1, rest], wy_s.at[step - 1])
                    sent(hid.at[many, 0], hy_s.at[step - 1])

            @pl.when(me_z != end * (nz - 1))
            def _():
                sent(z_in.at[many, 0, first], z_s.at[end])
                sent(z_in.at[many, :, rest], wz_s.at[end])
                for step in range(1, ny):
                    sent(hid.at[many, 0, own], ny_s.at[end, step - 1])

            @pl.when(me_z != (1 - end) * (nz - 1))
            def _():
                sent(hid.at[many, :, both], hz_s.at[end])
                sent(hid.at[many, 0, own], nz_s.at[end])

    def half_of(which):
        return pl.ds(pl.multiple_of(which * half_rows, half_rows), half_rows)

    def core_sum(layer, g):
        c_out[layer, g] = acc[g, half_of(1 - core), :].astype(BF16)
        core_copy(layer, g).start()

    def chip_sum(layer, g):
        core_copy(layer, g).wait()
        value = acc[g, half_of(core), :] + c_in[layer, g].astype(F32)
        c_sum[layer, g, chip] = value.astype(BF16)
        for step in range(1, chips):
            sum_copy(layer, g, step, chip).start()

    def total_sum(layer, g):
        for step in range(1, chips):
            sum_copy(layer, g, step, lax.rem(chip - step + chips, chips)).wait_recv()
            sum_copy(layer, g, step, chip).wait_send()
        value = c_sum[layer, g, 0].astype(F32)
        for other in range(1, chips):
            value = value + c_sum[layer, g, other].astype(F32)
        c_all[layer, g, core] = value.astype(BF16)
        all_copy(layer, g, core).start()

    def out_copy(g):
        return pltpu.make_async_copy(out_ref.at[g], out_hbm.at[g], o_sem.at[g])

    def finish(layer, g):
        all_copy(layer, g, 1 - core).wait_recv()
        all_copy(layer, g, core).wait_send()
        settle_squares(layer, g)
        branch = c_all[layer, g].reshape(rows, c_all.shape[4]).astype(F32)
        carried[g] = RESID * carried[g] + branch

        @pl.when(layer < layers - 1)
        def _():
            prepare(layer + 1, g)
            send_squares(layer + 1, g)

        @pl.when(layer == layers - 1)
        def _():
            out_ref[g] = carried[g].astype(out_ref.dtype)
            out_copy(g).start()

    def enter(g):
        carried[g] = tok_ref[g].astype(F32)
        prepare(0, g)

    for copy in inputs:
        copy.wait()
    enter(0)
    pl.semaphore_wait(barrier, guests)
    send_squares(0, 0)

    act_lag = LAG_Y + LAG_Z * (nz - 1)
    gather_lag = act_lag + LAG_HY
    down_lag = gather_lag + LAG_HZ * (nz - 1)
    total_lag = down_lag + TAIL_END
    stride = max(per_layer, chunks + total_lag)
    stride += stride % 2
    gap = stride - per_layer

    def body(t, _):
        odd = lax.rem(t, 2)
        towards = odd, 1 - odd
        hops = [jnp.where(end == 0, nz - 1 - me_z, me_z) for end in towards]

        def place(lag):
            spot = t - lag
            layer = 0
            for other in range(1, layers):
                layer = layer + jnp.where(spot >= other * stride, 1, 0)
            at = spot - layer * gap
            active = (spot >= 0) & (at < (layer + 1) * per_layer)
            return active, at, towards[lag % 2], hops[lag % 2], layer

        def split_up(at, layer):
            q = at - layer * per_layer
            g = lax.div(q, chunks)
            return g, q - g * chunks

        for lag, stage in ((TAIL_END, finish), (TAIL_SUM, total_sum), (TAIL_CHIP, chip_sum)):
            active, at, end, hop, layer = place(down_lag + lag)

            @pl.when(active)
            def _():
                g, i = split_up(at, layer)

                @pl.when(i == chunks - 1)
                def _():
                    stage(layer, g)

        active, at, end, hop, layer = place(0)

        @pl.when(active)
        def _():
            g, i = split_up(at, layer)

            @pl.when((layer == 0) & (i == 0) & (g > 0))
            def _():
                enter(g)
                send_squares(0, g)

            project(layer, g, i, at, end, hop)

        for far in range(nz - 1, 0, -1):
            active, at, end, hop, layer = place(act_lag + LAG_HZ * far)

            @pl.when(active & (hop == nz - 1 - far))
            def _():
                own_copy(at, end).wait_recv()
                if far < nz - 1:
                    own_copy(at, end).start()
                for step in range(1, ny):
                    cross_copy(at, end, step, me_y).start()

        for far in range(nz - 2, 0, -1):
            active, at, end, hop, layer = place(gather_lag + LAG_HZ * far)

            @pl.when(active & (hop == nz - 1 - far))
            def _():
                hz_copy(at, end).wait_recv()
                hz_copy(at, end).start()

        active, at, end, hop, layer = place(gather_lag)

        @pl.when(active & (hop == nz - 1))
        def _():
            gather_y(at)
            hz_copy(at, end).start()

        active, at, end, hop, layer = place(act_lag)

        @pl.when(active)
        def _():
            g, i = split_up(at, layer)

            @pl.when((i < 2) & (hop == nz - 1))
            def _():
                scale(layer, g, end)

            @pl.when(hop == nz - 1)
            def _():
                activate(layer, g, i, at, end)

        active, at, end, hop, layer = place(LAG_Z * (nz - 1))

        @pl.when(active & (hop == nz - 1))
        def _():
            add_wide(at, end)
            for step in range(1, ny):
                late_copy(at, step).start()

        for k in range(nz - 2, 0, -1):
            active, at, end, hop, layer = place(LAG_Z * k)

            @pl.when(active & (hop == k))
            def _():
                add_wide(at, end)
                wide_copy(at, end).start()

            active, at, end, hop, layer = place(LAG_Y + LAG_Z * k)

            @pl.when(active & (hop == k))
            def _():
                part[at, me_y, first] = add_z(at, end).astype(BF16)
                z_copy(at, end).start()
                g, i = split_up(at, layer)

                @pl.when(i < 2)
                def _():
                    sq_fwd[layer, g, end] = chain_squares(layer, g, end)
                    square_along(layer, g, end).start()

        active, at, end, hop, layer = place(LAG_Y)

        @pl.when(active)
        def _():
            part[at, me_y, first] = add_y(at, y_copy, first).astype(BF16)

            @pl.when(hop == 0)
            def _():
                z_copy(at, end).start()

            g, i = split_up(at, layer)

            @pl.when(i == 0)
            def _():
                add_squares(layer, g)

            @pl.when((i < 2) & (hop == 0))
            def _():
                sq_fwd[layer, g, end] = sq_sum[layer, g]
                square_along(layer, g, end).start()

        active, at, end, hop, layer = place(down_lag)

        @pl.when(active)
        def _():
            g, i = split_up(at, layer)

            @pl.when(hop == 0)
            def _():
                hz_copy(at, end).wait_recv()

            @pl.when(hop < nz - 1)
            def _():
                for step in range(1, ny):
                    cross_copy(at, end, step, lax.rem(me_y - step + ny, ny)).wait_recv()

            down(layer, g, i, at)

            @pl.when(i == chunks - 1)
            def _():
                core_sum(layer, g)

        return 0

    lax.fori_loop(0, stride * (layers - 1) + per_layer + total_lag, body, 0)
    settle()
    for g in range(groups):
        out_copy(g).wait()


def per_device(n_ra, n_cb, tokens, gain, gw, uw, gt, ut, gb, ub, dw):
    seqs, length, d = tokens.shape
    layers, _, ff = gw.shape
    nz = seqs
    ny = n_ra // nz
    blocks = ny if ff % (ny * LANES) == 0 else 1
    width = blocks * LANES
    groups = seqs * blocks // ny
    rows = seqs * length // groups
    chunks = ff // width
    n = layers * groups * chunks
    dims = (n_ra, n_cb, nz, groups, rows, length, layers, width, chunks)
    hbm = pl.BlockSpec(memory_space=pl.ANY)
    dma = pltpu.SemaphoreType.DMA
    ys = max(ny - 1, 1)
    half, chips = rows // CORES, n_cb // CORES
    taps = gt.shape[1]
    scratch = [
        pltpu.VMEM((groups, rows, d), tokens.dtype),
        pltpu.VMEM((groups, rows, d), tokens.dtype),
        pltpu.VMEM(gain.shape, F32),
        pltpu.VMEM((taps, layers, ff), F32),
        pltpu.VMEM((taps, layers, ff), F32),
        pltpu.VMEM(gb.shape, F32),
        pltpu.VMEM(ub.shape, F32),
        pltpu.VMEM((layers, d, ff), BF16),
        pltpu.VMEM((layers, d, ff), BF16),
        pltpu.VMEM((layers, ff, d), BF16),
        pltpu.VMEM((groups, rows, d), F32),
        pltpu.VMEM((groups, rows, d), BF16),
        pltpu.VMEM((groups, rows, LANES), F32),
        pltpu.VMEM((groups, rows, d), F32),
        pltpu.VMEM((layers, groups, 1, rows), F32),
        pltpu.VMEM((layers, groups, ys, 1, rows), F32),
        pltpu.VMEM((layers, groups, 1, rows), F32),
        pltpu.VMEM((layers, groups, 2, 1, rows), F32),
        pltpu.VMEM((layers, groups, 2, 1, rows), F32),
        pltpu.VMEM((n, ny, length, 2 * LANES), BF16),
        pltpu.VMEM((n, ys, length, 2 * LANES), BF16),
        pltpu.VMEM((n, ny, length, 2 * LANES), BF16),
        pltpu.VMEM((n, ny, length, LANES), BF16),
        pltpu.VMEM((layers, groups, half, d), BF16),
        pltpu.VMEM((layers, groups, half, d), BF16),
        pltpu.VMEM((layers, groups, chips, half, d), BF16),
        pltpu.VMEM((layers, groups, CORES, half, d), BF16),
        dma((groups,)), dma((6,)),
        dma((layers, chunks, 3)),
        dma((layers, groups, ys)), dma((layers, groups, ys)),
        dma((layers, groups, 2)), dma((layers, groups, 2)),
        dma((ys,)), dma((n, ys)),
        dma((2,)), dma((n,)),
        dma((2,)), dma((n,)),
        dma((ys,)), dma((n, ys)),
        dma((ys,)), dma((n, ys)),
        dma((2,)), dma((n,)),
        dma((2,)), dma((n,)),
        dma((2, ys)), dma((n, ys)),
        dma((layers, groups)), dma((layers, groups)),
        dma((layers, groups, max(chips - 1, 1))), dma((layers, groups, max(chips - 1, 1))),
        dma((layers, groups)), dma((layers, groups)),
    ]
    out = pl.pallas_call(
        functools.partial(kernel, dims),
        out_shape=jax.ShapeDtypeStruct((groups, rows, d), tokens.dtype),
        in_specs=[hbm] * 9,
        out_specs=hbm,
        scratch_shapes=scratch,
        compiler_params=pltpu.CompilerParams(
            collective_id=0, has_side_effects=True, vmem_limit_bytes=60 * 1024 * 1024
        ),
        name="blocks",
    )(
        tokens.reshape(groups, rows, d), gain, gw, uw,
        jnp.transpose(gt, (1, 0, 2)), jnp.transpose(ut, (1, 0, 2)), gb, ub, dw,
    )
    return out.reshape(tokens.shape)


def solution(mesh):
    in_specs = (
        P(None, None, "ra"),
        P(None, "ra"),
        P(None, "ra", "cb"),
        P(None, "ra", "cb"),
        P(None, None, "cb"),
        P(None, None, "cb"),
        P(None, "cb"),
        P(None, "cb"),
        P(None, "cb", "ra"),
    )
    return jax.shard_map(
        functools.partial(per_device, mesh.shape["ra"], mesh.shape["cb"]),
        mesh=mesh, in_specs=in_specs, out_specs=P(None, None, "ra"), check_vma=False,
    )
```
